128 devices in a mesh: sp: 64 (over z, y, x), tp: 2 (over core).
Axes of the slice: x: 4, y: 4, z: 4, core: 2. Of those that a mesh axis runs over, the one named last changes fastest.
Arguments:
- latent: bfloat16 [16384, 256], P('sp'), may hold values from -6 to 6
- rotary_key: bfloat16 [16384, 64], P('sp'), may hold values from -7 to 7
- doc_ids: int32 [16384], P('sp'), may hold values from 0 to 31, never falling along the last dimension, each value on 1 to 1024 neighbouring positions
- queries_content: bfloat16 [16384, 1024], P('sp', 'tp'), may hold values from -6 to 6
- queries_rotary: bfloat16 [16384, 512], P('sp', 'tp'), may hold values from -400 to 400
- w_key_up: bfloat16 [256, 1024], replicated, may hold values from -0.375 to 0.375
- w_value_up: bfloat16 [256, 1024], replicated, may hold values from -0.375 to 0.375
- w_out: bfloat16 [1024, 2048], P('tp'), may hold values from -1.5 to 1.5
- residual: bfloat16 [16384, 2048], P(('sp', 'tp')), may hold values from -4 to 4
- norm_gain: float32 [2048], replicated, may hold values from 0.1 to 1.9
- routes: int32 [16384, 2], P(('sp', 'tp')), may hold values from 0 to 63, all different within a row; in each aligned block of 128 rows (0 to 127, 128 to 255, ...) at most 8 rows name the same one
- route_weights: float32 [16384, 2], P(('sp', 'tp')), may hold values from 0.1 to 1
- w_gate: bfloat16 [64, 2048, 3584], P('sp', None, 'tp'), may hold values from -0.125 to 0.125
- w_up: bfloat16 [64, 2048, 3584], P('sp', None, 'tp'), may hold values from -0.125 to 0.125
- w_down: bfloat16 [64, 3584, 2048], P('sp', 'tp'), may hold values from -0.09375 to 0.09375
- out_gain: float32 [2048], replicated, may hold values from 0.1 to 1.9
Outputs:
- mixed: bfloat16 [16384, 2048], P(('sp', 'tp'))
The draws below stay inside these ranges and needn't reach their ends.
Inputs may be any that keep to these rules, and one draw needn't show every extreme that they name: `doc_ids`: document numbers never fall along positions; each document holds 1 to 1024 positions, and one holds exactly 1024. `routes`: each row names 2 different experts; among the rows of one device (aligned blocks of 128 rows) no expert is named more than 8 times, and in some blocks one expert is named exactly 8 times.
All inputs are finite; a program needn't handle non-finite values.
Results may differ from the reference program's by a relative error of at most 0.014.
Values may be sent and summed in bfloat16 or wider, within the bound.
A program may use at most 128 MiB of HBM per device.

```python
import math
import jax
import jax.numpy as jnp
import numpy as np
from jax import lax

D = 2048
HEADS = 8
DK = 128
DR = 64
DV = 128
RANK = 256
FF = 3584
TOPK = 2
REACH = 4
TOK_DEV = 256
TOKENS = 16384
ROWS = 128
EXPERTS = 64
CAP = 8
DOCS = 32
DOC_MOST = 1024
N_SP = 64
N_TP = 2


def rotary_base(key):
    rotary_draw = jnp.clip(jax.random.normal(jax.random.fold_in(key, 7), (TOKENS, DR), jnp.float32), -4.5, 4.5)
    return rotary_draw


def draw_rotary_key(key, part):
    return rotary_base(key).astype(jnp.bfloat16)


def draw_queries_rotary(key, part):
    drawn = jax.random.normal(jax.random.fold_in(key, 8), (TOKENS, HEADS, DR), jnp.float32)
    return drawn.reshape(TOKENS, HEADS * DR).astype(jnp.bfloat16)


def levels(stream_key, shape, cuts, smallest, high):
    gain = 1.0
    for dim, shards_of in cuts:
        steps = jax.random.uniform(jax.random.fold_in(jax.random.fold_in(stream_key, 6), dim), (shards_of,), jnp.float32, smallest / len(cuts), high / len(cuts))
        gain = gain * jnp.repeat(jnp.exp(steps), shape[dim] // shards_of).reshape((-1,) + (1,) * (len(shape) - 1 - dim))
    return gain


def split_up(amount, total, limit, skew):
    loads = [(1 << 20) // math.isqrt(rank ** skew) + 1 for rank in range(2, amount + 1)]
    rest, holding = total - limit - (amount - 1), [1] * (amount - 1)
    while rest > 0:
        movable = [i for i in range(amount - 1) if holding[i] < limit]
        mass, budget = sum([loads[i] for i in movable]), rest
        for i in movable:
            addition = min(limit - holding[i], max(1, budget * loads[i] // mass), rest)
            holding[i] = holding[i] + addition
            rest = rest - addition
    return np.array([limit] + holding)


def uneven(own_key, amount, total, bound, lean):
    if amount == 2:
        one = jax.random.randint(own_key, (), max(1, total - bound), min(bound, total - 1) + 1)
        return jnp.stack([one, total - one])
    tallies = jnp.asarray(split_up(amount, total, bound, lean), jnp.int32)
    couples = (amount - 1) // 2
    donor, sink = tallies[1:1 + 2 * couples:2], tallies[2:2 + 2 * couples:2]
    room = jnp.minimum(donor - 1, bound - sink)
    moved = jax.random.randint(jax.random.fold_in(own_key, 1), (couples,), 0, 1 << 20) % (room + 1)
    tallies = tallies.at[1:1 + 2 * couples:2].set(donor - moved).at[2:2 + 2 * couples:2].set(sink + moved)
    return tallies[jax.random.permutation(jax.random.fold_in(own_key, 2), amount)]


def assign_block(stream_key, own, number, rows, number_of, top, most, lean):
    ranking = jax.random.permutation(stream_key, number_of)
    heavy_load, ordinary = shares(number_of, rows * top, most, lean, True), shares(number_of, rows * top, most, lean, False)
    places = jnp.arange(number_of)

    def named(tallies, turn):
        used = int((tallies > 0).sum())
        fixed = max(1, used // 4)
        shifted = fixed + (places - fixed + turn * (used - fixed)) % max(1, number_of - fixed)
        return jnp.zeros((number_of,), jnp.int32).at[ranking[jnp.where(places < fixed, places, shifted)]].set(jnp.asarray(tallies, jnp.int32))

    tallies = jnp.where(number % 4 == 0, named(heavy_load, number // 4), named(ordinary, number - number // 4 - 1))
    mixed = jax.random.permutation(jax.random.fold_in(own, 3), number_of)
    donor, receiver = mixed[0:number_of // 2 * 2:2], mixed[1:number_of // 2 * 2:2]
    room = jnp.minimum(tallies[donor] - 1, most - tallies[receiver]) // 2
    room = jnp.where((donor == ranking[0]) | (receiver == ranking[0]) | (tallies[receiver] == 0), 0, jnp.maximum(room, 0))
    shifted = jax.random.randint(jax.random.fold_in(own, 4), (number_of // 2,), 0, 1 << 20) % (room + 1)
    tallies = tallies.at[donor].add(-shifted).at[receiver].add(shifted)
    labels = jnp.searchsorted(jnp.cumsum(tallies), jnp.arange(rows * top), side="right").astype(jnp.int32)
    listing = labels.reshape(top, rows).T
    listing = listing[jax.random.permutation(jax.random.fold_in(own, 1), rows)]
    turn = jax.random.randint(jax.random.fold_in(own, 2), (rows, 1), 0, top)
    return jnp.take_along_axis(listing, (jnp.arange(top)[None, :] + turn) % top, axis=1)


def shares(count, total, most, lean, full):
    weights = [(1 << 20) // math.isqrt(standing ** lean) + 1 for standing in range(1, count + 1)]
    largest = most if full else min(most, max(-(-total // count), total * weights[0] // sum(weights)))
    least = 1 if total - largest >= count - 1 else 0
    holding, rest = [largest] + [least] * (count - 1), total - largest - least * (count - 1)
    while rest > 0:
        candidates = [i for i in range(1, count) if holding[i] < largest] or [i for i in range(1, count) if holding[i] < most]
        pool, budget = sum([weights[i] for i in candidates]), rest
        for i in candidates:
            more = min(most - holding[i], max(1, budget * weights[i] // pool), rest)
            holding[i] = holding[i] + more
            rest = rest - more
    return np.array(holding)


def normal_values(rng, shape, width, limit, shards=(), held_as=jnp.bfloat16):
    entries = jax.random.normal(rng, shape, jnp.float32) * width
    if len(shards) > 0:
        entries = levels(rng, shape, shards, -0.22, 0.18) * entries
    return jnp.clip(entries, min=-limit, max=limit).astype(held_as)


def setup_inputs(seed: int = 0) -> dict:
    keys = jax.random.split(jax.random.key(seed), 17)
    latent = normal_values(keys[0], (TOKENS, RANK), 1.0, 6.0, ((0, 64),))
    rotary_key = draw_rotary_key(jax.random.fold_in(keys[16], 71), 0)
    doc_ids = jnp.searchsorted(jnp.cumsum(uneven(keys[2], DOCS, TOKENS, DOC_MOST, 2)), jnp.arange(TOKENS), side="right").astype(jnp.int32)
    queries_content = normal_values(keys[3], (TOKENS, HEADS * DK), 1.0, 6.0, ((0, 64), (1, 2)))
    queries_rotary = draw_queries_rotary(jax.random.fold_in(keys[16], 71), 0)
    w_key_up = normal_values(keys[5], (RANK, HEADS * DK), RANK ** -0.5, 0.375)
    w_value_up = normal_values(keys[6], (RANK, HEADS * DV), RANK ** -0.5, 0.375)
    w_out = normal_values(keys[7], (HEADS * DV, D), (HEADS * DV // 64) ** -0.5, 1.5, ((0, 2),))
    residual = normal_values(keys[8], (TOKENS, D), 0.5, 4.0, ((0, 128),))
    norm_gain = jnp.clip(1.0 + 0.18 * jax.random.normal(keys[9], (D,), jnp.float32), 0.1, 1.9)
    routes_keys = jax.random.split(jax.random.fold_in(keys[10], 1), TOKENS // ROWS)
    routes_turns = jax.random.permutation(jax.random.fold_in(keys[10], 3), TOKENS // ROWS)
    routes = jax.vmap(lambda own, number: assign_block(jax.random.fold_in(keys[10], 2), own, number, ROWS, EXPERTS, TOPK, CAP, 2))(routes_keys, routes_turns).reshape((TOKENS, TOPK))
    route_weights = jnp.clip(0.1 + 0.9 * jax.random.uniform(keys[11], (TOKENS, TOPK), jnp.float32) ** levels(keys[11], (TOKENS, TOPK), ((0, 128),), -0.2, 0.2), 0.1, 1.0)
    w_gate = normal_values(keys[12], (EXPERTS, D, FF), D ** -0.5, 0.125, ((0, 64), (2, 2)))
    w_up = normal_values(keys[13], (EXPERTS, D, FF), D ** -0.5, 0.125, ((0, 64), (2, 2)))
    w_down = normal_values(keys[14], (EXPERTS, FF, D), FF ** -0.5, 0.09375, ((0, 64), (1, 2)))
    out_gain = jnp.clip(1.0 + 0.18 * jax.random.normal(keys[15], (D,), jnp.float32), 0.1, 1.9)
    return {"latent": latent, "rotary_key": rotary_key, "doc_ids": doc_ids, "queries_content": queries_content, "queries_rotary": queries_rotary, "w_key_up": w_key_up, "w_value_up": w_value_up, "w_out": w_out, "residual": residual, "norm_gain": norm_gain, "routes": routes, "route_weights": route_weights, "w_gate": w_gate, "w_up": w_up, "w_down": w_down, "out_gain": out_gain}


ROPE_THETA = 500000.0
RESIDUAL_SCALE = 2.0 ** 0.5
NORM_EPSILON = 1e-05

def rotate(values, positions):
    half_width = values.shape[-1] // 2
    frequency = ROPE_THETA ** (-2.0 * jnp.arange(half_width, dtype=jnp.float32) / values.shape[-1])
    angles = positions.astype(jnp.float32)[:, None] * frequency[None, :]
    table_shape = (values.shape[0],) + (1,) * (values.ndim - 2) + (half_width,)
    cosine = jnp.cos(angles).reshape(table_shape)
    sine_part = jnp.sin(angles).reshape(table_shape)
    widened = values.astype(jnp.float32)
    first_half = widened[..., :half_width]
    second = widened[..., half_width:]
    return jnp.concatenate([first_half * cosine - second * sine_part, second * cosine + first_half * sine_part], -1)

def layer_norm(values, gain_vec):
    centre = lax.optimization_barrier(jnp.mean(values, -1, keepdims=True))
    spread = lax.optimization_barrier(jnp.mean(jnp.square(values - centre), -1, keepdims=True))
    return (values - centre) * lax.rsqrt(spread + NORM_EPSILON) * gain_vec

def reference(latent, rotary_key, doc_ids, queries_content, queries_rotary, w_key_up, w_value_up, w_out, residual, norm_gain, routes, route_weights, w_gate, w_up, w_down, out_gain):
    positions = jnp.arange(TOKENS, dtype=jnp.int32)
    key_content = jnp.dot(latent, w_key_up, preferred_element_type=jnp.float32).astype(jnp.bfloat16)
    key_content = key_content.reshape(TOKENS, HEADS, DK)
    values = jnp.dot(latent, w_value_up, preferred_element_type=jnp.float32).astype(jnp.bfloat16)
    values = values.reshape(TOKENS, HEADS, DV)
    key_rotary = rotate(rotary_key, positions).astype(jnp.bfloat16)
    query_rotary = rotate(queries_rotary.reshape(TOKENS, HEADS, DR), positions).astype(jnp.bfloat16)
    query_content = queries_content.reshape(TOKENS, HEADS, DK)
    padding = REACH * TOK_DEV
    key_pad = jnp.concatenate([jnp.zeros((padding, HEADS, DK), jnp.bfloat16), key_content], 0)
    value_pad = jnp.concatenate([jnp.zeros((padding, HEADS, DV), jnp.bfloat16), values], 0)
    rotary_pad = jnp.concatenate([jnp.zeros((padding, DR), jnp.bfloat16), key_rotary], 0)
    doc_pad = jnp.concatenate([jnp.full((padding,), -1, jnp.int32), doc_ids.astype(jnp.int32)], 0)
    position_pad = jnp.arange(TOKENS + padding, dtype=jnp.int32) - padding
    score_scale = (DK + DR) ** (-0.5)
    window = padding + TOK_DEV

    def attend_block(block_start):
        key_window = lax.dynamic_slice_in_dim(key_pad, block_start, window, 0).astype(jnp.float32)
        value_window = lax.dynamic_slice_in_dim(value_pad, block_start, window, 0).astype(jnp.float32)
        rotary_window = lax.dynamic_slice_in_dim(rotary_pad, block_start, window, 0).astype(jnp.float32)
        doc_window = lax.dynamic_slice_in_dim(doc_pad, block_start, window, 0)
        key_position = lax.dynamic_slice_in_dim(position_pad, block_start, window, 0)
        query_block = lax.dynamic_slice_in_dim(query_content, block_start, TOK_DEV, 0).astype(jnp.float32)
        turned_block = lax.dynamic_slice_in_dim(query_rotary, block_start, TOK_DEV, 0).astype(jnp.float32)
        query_doc = lax.dynamic_slice_in_dim(doc_ids.astype(jnp.int32), block_start, TOK_DEV, 0)
        query_position = lax.dynamic_slice_in_dim(positions, block_start, TOK_DEV, 0)
        scores = jnp.einsum('phd,qhd->hpq', query_block, key_window)
        scores = (scores + jnp.einsum('phd,qd->hpq', turned_block, rotary_window)) * score_scale
        allowed = (key_position[None, :] <= query_position[:, None]) & (key_position[None, :] >= 0)
        allowed = allowed & (doc_window[None, :] == query_doc[:, None])
        scores = jnp.where(allowed[None], scores, -jnp.inf)
        row_peak = lax.optimization_barrier(jnp.max(scores, -1, keepdims=True))
        lifted = jnp.exp(scores - row_peak)
        probability = (lifted / lax.optimization_barrier(jnp.sum(lifted, -1, keepdims=True))).astype(jnp.bfloat16)
        result = jnp.einsum('hpq,qhd->phd', probability.astype(jnp.float32), value_window)
        return result.astype(jnp.bfloat16)
    starts = jnp.arange(N_SP, dtype=jnp.int32) * TOK_DEV
    attended = lax.map(attend_block, starts).reshape(TOKENS, HEADS * DV)
    head_cols = HEADS * DV // N_TP
    projected = jnp.zeros((TOKENS, D), jnp.float32)
    for group in range(N_TP):
        partial_value = jnp.dot(attended[:, group * head_cols:(group + 1) * head_cols], w_out[group * head_cols:(group + 1) * head_cols], preferred_element_type=jnp.float32)
        projected = projected + partial_value.astype(jnp.bfloat16).astype(jnp.float32)
    normed = layer_norm(RESIDUAL_SCALE * residual.astype(jnp.float32) + projected, norm_gain).astype(jnp.bfloat16)
    capacity_all = N_SP * N_TP * CAP
    half_cols = FF // N_TP
    expert_ids = jnp.arange(EXPERTS, dtype=jnp.int32)

    def add_expert(running, inputs):
        expert_id, gate_w, up_w, down_w = inputs
        chosen = routes == expert_id
        member = jnp.any(chosen, 1)
        weight = lax.optimization_barrier(jnp.sum(jnp.where(chosen, route_weights, 0.0), 1))
        token_index = jnp.nonzero(member, size=capacity_all, fill_value=0)[0].astype(jnp.int32)
        live_mask = (jnp.arange(capacity_all) < jnp.sum(member.astype(jnp.int32))).astype(jnp.float32)
        token_rows = normed[token_index]
        gate_pre = jnp.dot(token_rows, gate_w, preferred_element_type=jnp.float32)
        upward = jnp.dot(token_rows, up_w, preferred_element_type=jnp.float32)
        hidden = (jax.nn.silu(gate_pre) * upward).astype(jnp.bfloat16)
        summed = jnp.zeros((capacity_all, D), jnp.float32)
        for group in range(N_TP):
            partial_value = jnp.dot(hidden[:, group * half_cols:(group + 1) * half_cols], down_w[group * half_cols:(group + 1) * half_cols], preferred_element_type=jnp.float32)
            summed = summed + partial_value.astype(jnp.bfloat16).astype(jnp.float32)
        expert_out = summed.astype(jnp.bfloat16).astype(jnp.float32)
        contribution = expert_out * (weight[token_index] * live_mask)[:, None]
        return (running.at[token_index].add(contribution), None)
    routed_sum, _ = lax.scan(add_expert, jnp.zeros((TOKENS, D), jnp.float32), (expert_ids, w_gate, w_up, w_down))
    combined = RESIDUAL_SCALE * normed.astype(jnp.float32) + routed_sum
    return layer_norm(combined, out_gain).astype(jnp.bfloat16)
```

```python
import functools

import jax
import jax.numpy as jnp
from jax import lax
from jax.experimental import pallas as pl
from jax.experimental.pallas import tpu as pltpu
from jax.sharding import PartitionSpec as P

HEADS = 8
DK = 128
DR = 64
DV = 128
TOPK = 2
REACH = 4
RANK = 256
D = 2048
TOK = 256
ROWS = 128
FFH = 1792
CAP = 8
GROUPS = 4
PEERS = 16
LOCAL_HEADS = 4
CHIPS = 64

ROPE_THETA = 500000.0
RESIDUAL_SCALE = 2.0**0.5
NORM_EPSILON = 1e-05
EXCLUDED = -1e30
MESH = pl.DeviceIdType.MESH
VMEM_LIMIT = 67_000_000
F32 = jnp.float32
BF16 = jnp.bfloat16


def remote(src, dst, send, recv, chip, core):
    return pltpu.make_async_remote_copy(
        src_ref=src, dst_ref=dst, send_sem=send, recv_sem=recv, device_id=(chip, core), device_id_type=MESH
    )


def layer_norm(values, gain_vec):
    centre = jnp.mean(values, -1, keepdims=True)
    spread = jnp.mean(jnp.square(values - centre), -1, keepdims=True)
    return (values - centre) * lax.rsqrt(spread + NORM_EPSILON) * gain_vec


def attention_kernel(
    msg,
    qc,
    qaux,
    wk_hbm,
    wv_hbm,
    wo_hbm,
    residual,
    gain,
    out,
    kv,
    wk,
    wv,
    wo,
    scores,
    vals,
    att,
    psend,
    precv,
    wsem,
    ssem,
    rsem,
    fssem,
    frsem,
    psem,
):
    sp = lax.axis_index("sp")
    tp = lax.axis_index("tp")
    other = 1 - tp
    half = LOCAL_HEADS * DK
    cols = pl.ds(pl.multiple_of(tp * half, half), half)
    loads = [
        pltpu.make_async_copy(wk_hbm.at[:, cols], wk, wsem.at[0]),
        pltpu.make_async_copy(wv_hbm.at[:, cols], wv, wsem.at[1]),
        pltpu.make_async_copy(wo_hbm, wo, wsem.at[2]),
    ]
    for load in loads:
        load.start()
    barrier = pltpu.get_barrier_semaphore()
    for step in (1, 2, 3, 4, -1, -2, -3, -4):
        pl.semaphore_signal(
            barrier, inc=1, device_id=(lax.rem(sp + step + CHIPS, CHIPS), tp), device_id_type=MESH
        )
    pl.semaphore_signal(barrier, inc=1, device_id=(sp, other), device_id_type=MESH)
    pl.semaphore_wait(barrier, 2 * REACH + 1)

    mine = pl.ds(pl.multiple_of(tp * ROWS, ROWS), ROWS)
    sends = []
    for d in range(1, REACH + 1):
        sends.append(
            remote(
                msg.at[mine],
                kv.at[d - 1, tp],
                ssem.at[d - 1],
                rsem.at[d - 1],
                lax.rem(sp + d, CHIPS),
                tp,
            )
        )
        sends[-1].start()
    loads[0].wait()
    loads[1].wait()

    def block(rows, slot, causal):
        lat = rows[:, :RANK]
        aux = rows[:, RANK:]
        keys = jnp.dot(lat, wk[...], preferred_element_type=F32).astype(BF16)
        vals[pl.ds(slot * TOK, TOK), :] = jnp.dot(lat, wv[...], preferred_element_type=F32).astype(BF16)
        for h in range(LOCAL_HEADS):
            hs = slice(h * DK, (h + 1) * DK)
            query = jnp.concatenate([qc[:, hs], qaux[:, hs]], 1)
            key = jnp.concatenate([keys[:, hs], aux], 1)
            s = lax.dot_general(query, key, (((1,), (1,)), ((), ())), preferred_element_type=F32)
            if causal:
                r = lax.broadcasted_iota(jnp.int32, (TOK, TOK), 0)
                c = lax.broadcasted_iota(jnp.int32, (TOK, TOK), 1)
                s = jnp.where(c <= r, s, EXCLUDED)
            scores[h, :, slot * TOK : (slot + 1) * TOK] = s

    block(msg[...], 0, True)
    forwards = []
    for d in range(REACH):
        sends[d].wait_recv()
        forwards.append(remote(kv.at[d, tp], kv.at[d, tp], fssem.at[d], frsem.at[d], sp, other))
        forwards[-1].start()
        if d >= 1:
            remote(kv.at[d - 1, other], kv.at[d - 1, other], fssem.at[d - 1], frsem.at[d - 1], sp, other).wait_recv()
            block(kv[d - 1].reshape(TOK, RANK + 128), d, False)
    last = REACH - 1
    remote(kv.at[last, other], kv.at[last, other], fssem.at[last], frsem.at[last], sp, other).wait_recv()
    block(kv[last].reshape(TOK, RANK + 128), REACH, False)

    scale = (DK + DR) ** (-0.5)
    for h in range(LOCAL_HEADS):
        s = scores[h]
        peak = jnp.max(s, -1, keepdims=True)
        lifted = jnp.exp((s - peak) * scale)
        total = jnp.sum(lifted, -1, keepdims=True)
        hs = slice(h * DV, (h + 1) * DV)
        mixed = jnp.dot(lifted.astype(BF16), vals[:, hs], preferred_element_type=F32)
        att[:, hs] = (mixed / total).astype(BF16)
    loads[2].wait()
    theirs = pl.ds(pl.multiple_of(other * ROWS, ROWS), ROWS)
    psend[...] = jnp.dot(att[theirs, :], wo[...], preferred_element_type=F32).astype(BF16)
    swap = remote(psend, precv, psem.at[0], psem.at[1], sp, other)
    swap.start()
    own = jnp.dot(att[mine, :], wo[...], preferred_element_type=F32).astype(BF16).astype(F32)
    own = own + RESIDUAL_SCALE * residual[...].astype(F32)
    swap.wait_recv()
    out[...] = layer_norm(own + precv[...].astype(F32), gain[...]).astype(BF16)
    swap.wait_send()
    for d in range(REACH):
        sends[d].wait_send()
        forwards[d].wait_send()


def expert_kernel(
    normed,
    routes,
    weights,
    wg_hbm,
    wu_hbm,
    wd_hbm,
    gain,
    out,
    wg,
    wu,
    wd,
    obuf,
    xbuf,
    hid,
    ykeep,
    ysend,
    yrecv,
    ret,
    back,
    wsem,
    dsend,
    drecv,
    fsend,
    frecv,
    ysendsem,
    yrecvsem,
    bsend,
    brecv,
):
    sp = lax.axis_index("sp")
    tp = lax.axis_index("tp")
    other = 1 - tp
    loads = [
        pltpu.make_async_copy(wg_hbm.at[0], wg, wsem.at[0]),
        pltpu.make_async_copy(wu_hbm.at[0], wu, wsem.at[1]),
        pltpu.make_async_copy(wd_hbm.at[0], wd, wsem.at[2]),
    ]
    for load in loads:
        load.start()
    barrier = pltpu.get_barrier_semaphore()

    def greet(i, carry):
        pl.semaphore_signal(barrier, inc=1, device_id=(lax.rem(sp + i, CHIPS), tp), device_id_type=MESH)
        return carry

    lax.fori_loop(1, CHIPS, greet, 0)
    pl.semaphore_signal(barrier, inc=1, device_id=(sp, other), device_id_type=MESH)

    z, y, x = sp // 16, lax.rem(sp // 4, 4), lax.rem(sp, 4)
    lane = lax.broadcasted_iota(jnp.int32, (ROWS, 128), 1)
    picks = [routes[:, k : k + 1] for k in range(TOPK)]
    member = ((picks[0] == lane) | (picks[1] == lane)).astype(F32).astype(BF16)
    lower = (lane < lax.broadcasted_iota(jnp.int32, (ROWS, 128), 0)).astype(F32).astype(BF16)
    before = jnp.dot(lower, member, preferred_element_type=F32)
    slot_lane = lax.broadcasted_iota(jnp.int32, (ROWS, CHIPS * CAP), 1)
    gathers = []
    for pick in picks:
        rank = jnp.sum(jnp.where(pick == lane, before, 0.0), 1, keepdims=True).astype(jnp.int32)
        oz = lax.bitwise_and((pick >> 4) - z, 3)
        oy = lax.bitwise_and((pick >> 2) - y, 3)
        ox = lax.bitwise_and(pick - x, 3)
        place = lax.bitwise_and(oz + oy + ox, 3) * PEERS + oz * 4 + oy
        gathers.append((slot_lane == place * CAP + rank).astype(F32))
    placing = jnp.transpose(gathers[0] + gathers[1]).astype(BF16)
    gathers = [g.astype(BF16) for g in gathers]
    rows_in = normed[...]

    def there(g, j, sign):
        oz = j // 4
        oy = lax.rem(j, 4)
        ox = lax.rem(g + 8 - oz - oy, 4)
        dz = lax.rem(z + sign * oz + 4, 4)
        dy = lax.rem(y + sign * oy + 4, 4)
        dx = lax.rem(x + sign * ox + 4, 4)
        return dz * 16 + dy * 4 + dx

    pl.semaphore_wait(barrier, CHIPS)
    for g in range(GROUPS):
        obuf[g] = (
            jnp.dot(placing[g * ROWS : (g + 1) * ROWS], rows_in, preferred_element_type=F32)
            .astype(BF16)
            .reshape(PEERS, CAP, D)
        )
        first = 1 if g == 0 else 0

        def dispatch(j, carry, g=g):
            remote(obuf.at[g, j], xbuf.at[g, tp, j], dsend.at[g], drecv.at[g], there(g, j, 1), tp).start()
            return carry

        lax.fori_loop(first, PEERS, dispatch, 0)
        if g == 0:
            xbuf[0, tp, 0] = obuf[0, 0]

    def arrived(g):
        first = 1 if g == 0 else 0
        part = xbuf.at[g, tp, pl.ds(first, PEERS - first)]
        remote(part, part, dsend.at[g], drecv.at[g], sp, other).wait_recv()
        fwd = remote(xbuf.at[g, tp], xbuf.at[g, tp], fsend.at[g], frecv.at[g], sp, other)
        fwd.start()

    arrived(0)
    for g in range(GROUPS):
        theirs = xbuf.at[g, other]
        remote(theirs, theirs, fsend.at[g], frecv.at[g], sp, other).wait_recv()
        if g == 0:
            loads[0].wait()
            loads[1].wait()
        rows = xbuf.at[g]

        def upward(n, carry):
            cols = pl.ds(pl.multiple_of(n * 256, 256), 256)
            lhs = rows[...].reshape(TOK, D)
            gate = jnp.dot(lhs, wg[:, cols], preferred_element_type=F32)
            up = jnp.dot(lhs, wu[:, cols], preferred_element_type=F32)
            hid[:, cols] = (gate / (1.0 + jnp.exp(-gate)) * up).astype(BF16)
            return carry

        lax.fori_loop(0, FFH // 256, upward, 0)
        if g == 0:
            loads[2].wait()

        def downward(n, carry):
            cols = pl.ds(pl.multiple_of(n * 256, 256), 256)
            ysend[g, :, cols] = jnp.dot(
                hid[pl.ds(pl.multiple_of(other * ROWS, ROWS), ROWS), :], wd[:, cols], preferred_element_type=F32
            ).astype(BF16)
            ykeep[:, cols] = jnp.dot(
                hid[pl.ds(pl.multiple_of(tp * ROWS, ROWS), ROWS), :], wd[:, cols], preferred_element_type=F32
            ).astype(BF16)
            return carry

        lax.fori_loop(0, D // 256, downward, 0)
        swap = remote(ysend.at[g], yrecv.at[g], ysendsem.at[g], yrecvsem.at[g], sp, other)
        swap.start()
        if g + 1 < GROUPS:
            arrived(g + 1)
        swap.wait_recv()
        ret[g] = (ykeep[...].astype(F32) + yrecv[g].astype(F32)).astype(BF16).reshape(PEERS, CAP, D)
        first = 1 if g == 0 else 0

        def send_back(j, carry):
            remote(ret.at[g, j], back.at[g, j], bsend.at[g], brecv.at[g], there(g, j, -1), tp).start()
            return carry

        lax.fori_loop(first, PEERS, send_back, 0)
        if g == 0:
            back[0, 0] = ret[0, 0]

    combined = RESIDUAL_SCALE * normed[...].astype(F32)
    picked = [jnp.zeros((ROWS, D), F32) for _ in range(TOPK)]
    for g in range(GROUPS):
        first = 1 if g == 0 else 0
        part = back.at[g, pl.ds(first, PEERS - first)]
        remote(part, part, bsend.at[g], brecv.at[g], sp, other).wait_recv()
        landed = back[g].reshape(ROWS, D)
        for k in range(TOPK):
            picked[k] = picked[k] + jnp.dot(
                gathers[k][:, g * ROWS : (g + 1) * ROWS], landed, preferred_element_type=F32
            )
    for k in range(TOPK):
        combined = combined + picked[k] * weights[:, k : k + 1]
    out[...] = layer_norm(combined, gain[...]).astype(BF16)
    for g in range(GROUPS):
        first = 1 if g == 0 else 0
        part = obuf.at[g, pl.ds(first, PEERS - first)]
        remote(part, part, dsend.at[g], drecv.at[g], sp, other).wait_send()
        part = ret.at[g, pl.ds(first, PEERS - first)]
        remote(part, part, bsend.at[g], brecv.at[g], sp, other).wait_send()
        remote(xbuf.at[g, tp], xbuf.at[g, tp], fsend.at[g], frecv.at[g], sp, other).wait_send()
        remote(ysend.at[g], ysend.at[g], ysendsem.at[g], yrecvsem.at[g], sp, other).wait_send()


def in_vmem():
    return pl.BlockSpec(memory_space=pltpu.VMEM)


def in_hbm():
    return pl.BlockSpec(memory_space=pl.ANY)


DMA = pltpu.SemaphoreType.DMA


def attend(msg, qc, qaux, w_key_up, w_value_up, w_out, residual, gain):
    return pl.pallas_call(
        attention_kernel,
        out_shape=jax.ShapeDtypeStruct((ROWS, D), BF16),
        in_specs=[in_vmem()] * 3 + [in_hbm()] * 3 + [in_vmem()] * 2,
        out_specs=in_vmem(),
        scratch_shapes=[
            pltpu.VMEM((REACH, 2, ROWS, RANK + 128), BF16),
            pltpu.VMEM((RANK, LOCAL_HEADS * DK), BF16),
            pltpu.VMEM((RANK, LOCAL_HEADS * DV), BF16),
            pltpu.VMEM((LOCAL_HEADS * DV, D), BF16),
            pltpu.VMEM((LOCAL_HEADS, TOK, (REACH + 1) * TOK), F32),
            pltpu.VMEM(((REACH + 1) * TOK, LOCAL_HEADS * DV), BF16),
            pltpu.VMEM((TOK, LOCAL_HEADS * DV), BF16),
            pltpu.VMEM((ROWS, D), BF16),
            pltpu.VMEM((ROWS, D), BF16),
            DMA((3,)),
            DMA((REACH,)),
            DMA((REACH,)),
            DMA((REACH,)),
            DMA((REACH,)),
            DMA((2,)),
        ],
        compiler_params=pltpu.CompilerParams(
            collective_id=0, has_side_effects=True, vmem_limit_bytes=VMEM_LIMIT
        ),
    )(msg, qc, qaux, w_key_up, w_value_up, w_out, residual, gain)


def route_and_mix(normed, routes, route_weights, w_gate, w_up, w_down, gain):
    return pl.pallas_call(
        expert_kernel,
        out_shape=jax.ShapeDtypeStruct((ROWS, D), BF16),
        in_specs=[in_vmem()] * 3 + [in_hbm()] * 3 + [in_vmem()],
        out_specs=in_vmem(),
        scratch_shapes=[
            pltpu.VMEM((D, FFH), BF16),
            pltpu.VMEM((D, FFH), BF16),
            pltpu.VMEM((FFH, D), BF16),
            pltpu.VMEM((GROUPS, PEERS, CAP, D), BF16),
            pltpu.VMEM((GROUPS, 2, PEERS, CAP, D), BF16),
            pltpu.VMEM((TOK, FFH), BF16),
            pltpu.VMEM((ROWS, D), BF16),
            pltpu.VMEM((GROUPS, ROWS, D), BF16),
            pltpu.VMEM((GROUPS, ROWS, D), BF16),
            pltpu.VMEM((GROUPS, PEERS, CAP, D), BF16),
            pltpu.VMEM((GROUPS, PEERS, CAP, D), BF16),
            DMA((3,)),
        ]
        + [DMA((GROUPS,))] * 8,
        compiler_params=pltpu.CompilerParams(
            collective_id=1, has_side_effects=True, vmem_limit_bytes=VMEM_LIMIT
        ),
    )(normed, routes, route_weights, w_gate, w_up, w_down, gain)


def rotate(values, positions):
    half_width = values.shape[-1] // 2
    frequency = ROPE_THETA ** (-2.0 * jnp.arange(half_width, dtype=jnp.float32) / values.shape[-1])
    angles = positions.astype(jnp.float32)[:, None] * frequency[None, :]
    table_shape = (values.shape[0],) + (1,) * (values.ndim - 2) + (half_width,)
    cosine = jnp.cos(angles).reshape(table_shape)
    sine_part = jnp.sin(angles).reshape(table_shape)
    widened = values.astype(jnp.float32)
    first_half = widened[..., :half_width]
    second = widened[..., half_width:]
    return jnp.concatenate(
        [first_half * cosine - second * sine_part, second * cosine + first_half * sine_part], -1
    )


def per_device(
    latent,
    rotary_key,
    doc_ids,
    queries_content,
    queries_rotary,
    w_key_up,
    w_value_up,
    w_out,
    residual,
    norm_gain,
    routes,
    route_weights,
    w_gate,
    w_up,
    w_down,
    out_gain,
):
    sp_index = lax.axis_index("sp")
    own_position = sp_index * TOK + jnp.arange(TOK, dtype=jnp.int32)
    query_turned = rotate(queries_rotary.reshape(TOK, LOCAL_HEADS, DR), own_position).astype(BF16)
    key_turned = rotate(rotary_key, own_position).astype(BF16)
    doc = jnp.arange(64, dtype=jnp.int32)[None, :]
    same = doc == doc_ids[:, None]
    marks = same.astype(BF16)
    fence = jnp.where(same | (doc >= 32), 0.0, EXCLUDED).astype(BF16)
    msg = jnp.concatenate([latent, key_turned, marks], 1)
    fences = jnp.broadcast_to(fence[:, None, :], (TOK, LOCAL_HEADS, 64))
    qaux = jnp.concatenate([query_turned, fences], -1).reshape(TOK, LOCAL_HEADS * 128)
    normed = attend(
        msg, queries_content, qaux, w_key_up, w_value_up, w_out, residual, norm_gain.reshape(1, D)
    )
    return route_and_mix(normed, routes, route_weights, w_gate, w_up, w_down, out_gain.reshape(1, D))


def solution(mesh):
    return jax.shard_map(
        per_device,
        mesh=mesh,
        in_specs=(
            P("sp", None),
            P("sp", None),
            P("sp"),
            P("sp", "tp"),
            P("sp", "tp"),
            P(),
            P(),
            P("tp", None),
            P(("sp", "tp"), None),
            P(),
            P(("sp", "tp"), None),
            P(("sp", "tp"), None),
            P("sp", None, "tp"),
            P("sp", None, "tp"),
            P("sp", "tp", None),
            P(),
        ),
        out_specs=P(("sp", "tp"), None),
        check_vma=False,
    )
```

```python
import jax
import jax.numpy as jnp
import numpy as np
from jax import lax
from jax.experimental import pallas as pl
from jax.experimental.pallas import tpu as pltpu
from jax.sharding import PartitionSpec as P

HEADS = 8
DK = 128
DR = 64
DV = 128
TOPK = 2
REACH = 4
RANK = 256
D = 2048
TOK = 256
ROWS = 128
FFH = 1792
CAP = 8
GROUPS = 4
PEERS = 16
LOCAL_HEADS = 4
CHIPS = 64

ROPE_THETA = 500000.0
RESIDUAL_SCALE = 2.0**0.5
NORM_EPSILON = 1e-05
EXCLUDED = -1e30
LOG2E = 1.4426950408889634
MESH = pl.DeviceIdType.MESH
VMEM_LIMIT = 62_000_000
F32 = jnp.float32
BF16 = jnp.bfloat16


def remote(src, dst, send, recv, chip, core):
    return pltpu.make_async_remote_copy(
        src_ref=src, dst_ref=dst, send_sem=send, recv_sem=recv, device_id=(chip, core), device_id_type=MESH
    )


def layer_norm(values, gain_vec):
    centre = jnp.mean(values, -1, keepdims=True)
    spread = jnp.mean(jnp.square(values - centre), -1, keepdims=True)
    return (values - centre) * lax.rsqrt(spread + NORM_EPSILON) * gain_vec


def layer_kernel(
    latent,
    key_rot,
    doc_row,
    frequency,
    gain,
    routes,
    weights,
    last_gain,
    qc_hbm,
    qr_hbm,
    residual_hbm,
    wk_hbm,
    wv_hbm,
    wo_hbm,
    wg_hbm,
    wu_hbm,
    wd_hbm,
    out,
    qc,
    qr,
    residual,
    aux_out,
    qaux,
    kvl,
    kva,
    wk,
    wv,
    wo,
    peaks,
    sums,
    att,
    psend,
    precv,
    nrm,
    wg,
    wu,
    wd,
    obuf,
    xbuf,
    lhs,
    hid,
    ybuf,
    yrecv,
    back,
    wsem,
    ssem,
    rsem,
    fssem,
    frsem,
    psem,
    met,
    dsend,
    drecv,
    fsend,
    frecv,
    ysendsem,
    yrecvsem,
    bsend,
    brecv,
):
    sp = lax.axis_index("sp")
    tp = lax.axis_index("tp")
    other = 1 - tp
    barrier = pltpu.get_barrier_semaphore()

    def signal(semaphore, chip, core):
        pl.semaphore_signal(semaphore, inc=1, device_id=(chip, core), device_id_type=MESH)

    z, y, x = sp // 16, lax.rem(sp // 4, 4), lax.rem(sp, 4)
    y_ring = [z * 16 + lax.rem(y + e, 4) * 4 + x for e in (1, 2, 3)]
    z_ring = [lax.rem(z + e, 4) * 16 + y * 4 + x for e in (1, 2, 3)]
    x_ring = [z * 16 + y * 4 + lax.rem(x + e, 4) for e in (1, 2, 3)]
    near = [lax.rem(sp + e + CHIPS, CHIPS) for e in (1, 2, 3, 4, -1, -2, -3, -4)]
    for chip in near + x_ring + y_ring + z_ring:
        signal(barrier, chip, tp)
    signal(barrier, sp, other)

    half = LOCAL_HEADS * DK
    cols = pl.ds(pl.multiple_of(tp * half, half), half)
    loads = [
        pltpu.make_async_copy(wk_hbm.at[:, cols], wk, wsem.at[0]),
        pltpu.make_async_copy(wv_hbm.at[:, cols], wv, wsem.at[1]),
        pltpu.make_async_copy(wo_hbm, wo, wsem.at[2]),
        pltpu.make_async_copy(wg_hbm.at[0], wg, wsem.at[3]),
        pltpu.make_async_copy(wu_hbm.at[0], wu, wsem.at[4]),
        pltpu.make_async_copy(wd_hbm.at[0], wd, wsem.at[5]),
        pltpu.make_async_copy(qc_hbm, qc, wsem.at[6]),
        pltpu.make_async_copy(qr_hbm, qr, wsem.at[7]),
        pltpu.make_async_copy(residual_hbm, residual, wsem.at[8]),
    ]
    for k in (0, 1, 6, 7, 2, 8):
        loads[k].start()
    mine = pl.ds(pl.multiple_of(tp * ROWS, ROWS), ROWS)
    theirs = pl.ds(pl.multiple_of(other * ROWS, ROWS), ROWS)
    pl.semaphore_wait(barrier, 18)
    latent_sends = []
    for d in range(REACH):
        chip = lax.rem(sp + d + 1, CHIPS)
        latent_sends.append(remote(latent.at[mine], kvl.at[d, tp], ssem.at[0, d], rsem.at[0, d], chip, tp))
        latent_sends[-1].start()

    doc_lane = lax.broadcasted_iota(jnp.int32, (64, TOK), 0)
    marks = (doc_lane == doc_row[...]).astype(F32)
    natural = jnp.transpose(jnp.concatenate([key_rot[...].astype(F32), marks], 0))
    wide = lax.broadcasted_iota(jnp.int32, (TOK, 128), 1)
    content = wide < DR
    low_half = lax.rem(wide, DR) < DR // 2
    position = (sp * TOK + lax.broadcasted_iota(jnp.int32, (TOK, 128), 0)).astype(F32)
    angles = position * frequency[...]
    cos_table = jnp.cos(angles)
    sin_table = jnp.where(low_half, -jnp.sin(angles), jnp.sin(angles))

    def turned(v):
        swapped = jnp.where(low_half, pltpu.roll(v, 128 - DR // 2, 1), pltpu.roll(v, DR // 2, 1))
        return v * cos_table + swapped * sin_table

    aux_out[...] = jnp.where(content, turned(natural), natural).astype(BF16)
    aux_sends = []
    for d in range(REACH):
        chip = lax.rem(sp + d + 1, CHIPS)
        aux_sends.append(remote(aux_out.at[mine], kva.at[d, tp], ssem.at[1, d], rsem.at[1, d], chip, tp))
        aux_sends[-1].start()
    loads[7].wait()
    fence = jnp.where(wide < DR + 32, (natural - 1.0) * -EXCLUDED, 0.0)
    for pair in range(LOCAL_HEADS // 2):
        two = turned(qr[:, pair * 128 : (pair + 1) * 128].astype(F32))
        first = jnp.where(content, two, fence)
        second = jnp.where(content, pltpu.roll(two, DR, 1), fence)
        qaux[:, pair * 256 : pair * 256 + 128] = first.astype(BF16)
        qaux[:, pair * 256 + 128 : pair * 256 + 256] = second.astype(BF16)

    expert = lax.broadcasted_iota(jnp.int32, (128, ROWS), 0)
    picks = [routes[k : k + 1, :] for k in range(TOPK)]
    member = ((picks[0] == expert) | (picks[1] == expert)).astype(F32).astype(BF16)
    upper = (expert < lax.broadcasted_iota(jnp.int32, (128, ROWS), 1)).astype(F32).astype(BF16)
    before = jnp.dot(member, upper, preferred_element_type=F32)
    slots = []
    for pick in picks:
        rank = jnp.sum(jnp.where(pick == expert, before, 0.0), 0, keepdims=True)
        oz = lax.bitwise_and((pick >> 4) - z, 3)
        oy = lax.bitwise_and((pick >> 2) - y, 3)
        ox = lax.bitwise_and(pick - x, 3)
        place = lax.bitwise_and(oz + oy + ox, 3) * PEERS + oz * 4 + oy
        slots.append(place * CAP + rank.astype(jnp.int32))
    slot_sub = lax.broadcasted_iota(jnp.int32, (CHIPS * CAP, ROWS), 0)
    placing = ((slot_sub == slots[0]) | (slot_sub == slots[1])).astype(F32).astype(BF16)
    table = jnp.where(
        expert == 0,
        slots[0].astype(F32),
        jnp.where(
            expert == 1,
            slots[1].astype(F32),
            jnp.where(expert == 2, weights[0:1, :], jnp.where(expert == 3, weights[1:2, :], 0.0)),
        ),
    )
    by_row = jnp.transpose(table)
    slot_lane = lax.broadcasted_iota(jnp.int32, (ROWS, CHIPS * CAP), 1).astype(F32)
    gathers = [(slot_lane == by_row[:, k : k + 1]).astype(F32).astype(BF16) for k in range(TOPK)]
    shares = [by_row[:, TOPK + k : TOPK + k + 1] for k in range(TOPK)]

    for chip in y_ring:
        signal(met.at[0], chip, tp)
    loads[0].wait()
    loads[1].wait()
    loads[6].wait()
    for load in loads[3:6]:
        load.start()

    rate = (DK + DR) ** (-0.5) * LOG2E
    ones = jnp.ones((TOK, DV), BF16)

    def block(lat, aux, first):
        keys = jnp.dot(lat, wk[...], preferred_element_type=F32).astype(BF16)
        values = jnp.dot(lat, wv[...], preferred_element_type=F32).astype(BF16)
        for h in range(LOCAL_HEADS):
            hs = slice(h * DK, (h + 1) * DK)
            query = jnp.concatenate([qc[:, hs], qaux[:, hs]], 1)
            key = jnp.concatenate([keys[:, hs], aux], 1)
            s = lax.dot_general(query, key, (((1,), (1,)), ((), ())), preferred_element_type=F32)
            if first:
                r = lax.broadcasted_iota(jnp.int32, (TOK, TOK), 0)
                c = lax.broadcasted_iota(jnp.int32, (TOK, TOK), 1)
                s = jnp.where(c <= r, s, EXCLUDED)
            peak = jnp.max(s, -1, keepdims=True)
            if not first:
                was = peaks[h][:, :1]
                peak = jnp.maximum(peak, was)
            lifted = jnp.exp2((s - peak) * rate).astype(BF16)
            made = jnp.dot(lifted, jnp.concatenate([values[:, hs], ones], 1), preferred_element_type=F32)
            if not first:
                made = made + sums[h] * jnp.exp2((was - peak) * rate)
            peaks[h] = jnp.broadcast_to(peak, (TOK, 128))
            sums[h] = made

    block(latent[...], aux_out[...], True)
    pl.semaphore_wait(met.at[0], 3)
    for chip in z_ring:
        signal(met.at[1], chip, tp)

    def relays(d, core):
        return [
            remote(part.at[d, core], part.at[d, core], fssem.at[i, d], frsem.at[i, d], sp, other)
            for i, part in enumerate((kvl, kva))
        ]

    def process(d):
        for relay in relays(d, other):
            relay.wait_recv()
        block(kvl[d].reshape(TOK, RANK), kva[d].reshape(TOK, 128), False)

    for d in range(REACH):
        for send, relay in zip((latent_sends[d], aux_sends[d]), relays(d, tp)):
            send.wait_recv()
            relay.start()
        if d >= 1:
            process(d - 1)
    loads[2].wait()
    loads[8].wait()
    process(REACH - 1)

    for h in range(LOCAL_HEADS):
        att[:, h * DV : (h + 1) * DV] = (sums[h, :, :DV] / sums[h, :, DV:]).astype(BF16)
    psend[...] = jnp.dot(att[theirs, :], wo[...], preferred_element_type=F32).astype(BF16)
    swap = remote(psend, precv, psem.at[0], psem.at[1], sp, other)
    swap.start()
    own = jnp.dot(att[mine, :], wo[...], preferred_element_type=F32).astype(BF16).astype(F32)
    own = own + RESIDUAL_SCALE * residual[...].astype(F32)
    swap.wait_recv()
    rows_in = layer_norm(own + precv[...].astype(F32), gain[...]).astype(BF16)
    nrm[...] = rows_in

    def there(g, j, sign):
        oz = j // 4
        oy = lax.rem(j, 4)
        ox = lax.rem(g + 8 - oz - oy, 4)
        dz = lax.rem(z + sign * oz + 4, 4)
        dy = lax.rem(y + sign * oy + 4, 4)
        dx = lax.rem(x + sign * ox + 4, 4)
        return dz * 16 + dy * 4 + dx

    pl.semaphore_wait(met.at[1], 3)
    for g in range(GROUPS):
        obuf[g] = (
            jnp.dot(placing[g * ROWS : (g + 1) * ROWS], rows_in, preferred_element_type=F32)
            .astype(BF16)
            .reshape(PEERS, CAP, D)
        )
        first = 1 if g == 0 else 0

        def dispatch(j, carry, g=g):
            remote(obuf.at[g, j], xbuf.at[g, tp, j], dsend.at[g], drecv.at[g], there(g, j, 1), tp).start()
            return carry

        lax.fori_loop(first, PEERS, dispatch, 0)
        if g == 0:
            xbuf[0, tp, 0] = obuf[0, 0]

    def arrived(g):
        first = 1 if isinstance(g, int) and g == 0 else 0
        part = xbuf.at[g, tp, pl.ds(first, PEERS - first)]
        remote(part, part, dsend.at[g], drecv.at[g], sp, other).wait_recv()
        remote(xbuf.at[g, tp], xbuf.at[g, tp], fsend.at[g], frecv.at[g], sp, other).start()

    def swap_of(g):
        return remote(ybuf.at[g, other], yrecv.at[g], ysendsem.at[g], yrecvsem.at[g], sp, other)

    def finish(g):
        swap_of(g).wait_recv()
        ybuf[g, tp] = (ybuf[g, tp].astype(F32) + yrecv[g].astype(F32)).astype(BF16)

        def send_back(j, carry):
            remote(ybuf.at[g, tp, j], back.at[g, j], bsend.at[g], brecv.at[g], there(g, j, -1), tp).start()
            return carry

        lax.fori_loop(jnp.where(g == 0, 1, 0), PEERS, send_back, 0)

    arrived(0)
    for load in loads[3:6]:
        load.wait()

    def group(g, carry):
        part = xbuf.at[g, other]
        remote(part, part, fsend.at[g], frecv.at[g], sp, other).wait_recv()
        lhs[...] = xbuf[g].reshape(TOK, D)
        gate = jnp.dot(lhs[...], wg[...], preferred_element_type=F32)
        up = jnp.dot(lhs[...], wu[...], preferred_element_type=F32)
        hid[...] = (gate / (1.0 + jnp.exp(-gate)) * up).astype(BF16)

        @pl.when(g > 0)
        def _():
            finish(g - 1)

        @pl.when(g + 1 < GROUPS)
        def _():
            arrived(g + 1)

        made = jnp.dot(hid[...], wd[...], preferred_element_type=F32).astype(BF16)
        ybuf[g] = made.reshape(2, PEERS, CAP, D)
        swap_of(g).start()
        return carry

    lax.fori_loop(0, GROUPS, group, 0)
    finish(GROUPS - 1)
    back[0, 0] = ybuf[0, tp, 0]

    combined = RESIDUAL_SCALE * nrm[...].astype(F32)
    picked = [jnp.zeros((ROWS, D), F32) for _ in range(TOPK)]
    for g in range(GROUPS):
        first = 1 if g == 0 else 0
        part = back.at[g, pl.ds(first, PEERS - first)]
        remote(part, part, bsend.at[g], brecv.at[g], sp, other).wait_recv()
        landed = back[g].reshape(ROWS, D)
        for k in range(TOPK):
            picked[k] = picked[k] + jnp.dot(
                gathers[k][:, g * ROWS : (g + 1) * ROWS], landed, preferred_element_type=F32
            )
    for k in range(TOPK):
        combined = combined + picked[k] * shares[k]
    out[...] = layer_norm(combined, last_gain[...]).astype(BF16)

    swap.wait_send()
    for d in range(REACH):
        for copy in (latent_sends[d], aux_sends[d], *relays(d, tp)):
            copy.wait_send()
    for g in range(GROUPS):
        first = 1 if g == 0 else 0
        part = obuf.at[g, pl.ds(first, PEERS - first)]
        remote(part, part, dsend.at[g], drecv.at[g], sp, other).wait_send()
        part = ybuf.at[g, tp, pl.ds(first, PEERS - first)]
        remote(part, part, bsend.at[g], brecv.at[g], sp, other).wait_send()
        remote(xbuf.at[g, tp], xbuf.at[g, tp], fsend.at[g], frecv.at[g], sp, other).wait_send()
        swap_of(g).wait_send()


def in_vmem():
    return pl.BlockSpec(memory_space=pltpu.VMEM)


def in_hbm():
    return pl.BlockSpec(memory_space=pltpu.HBM)


DMA = pltpu.SemaphoreType.DMA


def layer(*operands):
    return pl.pallas_call(
        layer_kernel,
        out_shape=jax.ShapeDtypeStruct((ROWS, D), BF16),
        in_specs=[in_vmem()] * 8 + [in_hbm()] * 9,
        out_specs=in_vmem(),
        scratch_shapes=[
            pltpu.VMEM((TOK, LOCAL_HEADS * DK), BF16),
            pltpu.VMEM((TOK, LOCAL_HEADS * DR), BF16),
            pltpu.VMEM((ROWS, D), BF16),
            pltpu.VMEM((TOK, 128), BF16),
            pltpu.VMEM((TOK, LOCAL_HEADS * 128), BF16),
            pltpu.VMEM((REACH, 2, ROWS, RANK), BF16),
            pltpu.VMEM((REACH, 2, ROWS, 128), BF16),
            pltpu.VMEM((RANK, LOCAL_HEADS * DK), BF16),
            pltpu.VMEM((RANK, LOCAL_HEADS * DV), BF16),
            pltpu.VMEM((LOCAL_HEADS * DV, D), BF16),
            pltpu.VMEM((LOCAL_HEADS, TOK, 128), F32),
            pltpu.VMEM((LOCAL_HEADS, TOK, 2 * DV), F32),
            pltpu.VMEM((TOK, LOCAL_HEADS * DV), BF16),
            pltpu.VMEM((ROWS, D), BF16),
            pltpu.VMEM((ROWS, D), BF16),
            pltpu.VMEM((ROWS, D), BF16),
            pltpu.VMEM((D, FFH), BF16),
            pltpu.VMEM((D, FFH), BF16),
            pltpu.VMEM((FFH, D), BF16),
            pltpu.VMEM((GROUPS, PEERS, CAP, D), BF16),
            pltpu.VMEM((GROUPS, 2, PEERS, CAP, D), BF16),
            pltpu.VMEM((TOK, D), BF16),
            pltpu.VMEM((TOK, FFH), BF16),
            pltpu.VMEM((GROUPS, 2, PEERS, CAP, D), BF16),
            pltpu.VMEM((GROUPS, PEERS, CAP, D), BF16),
            pltpu.VMEM((GROUPS, PEERS, CAP, D), BF16),
            DMA((9,)),
        ]
        + [DMA((2, REACH))] * 4
        + [DMA((2,)), pltpu.SemaphoreType.REGULAR((2,))]
        + [DMA((GROUPS,))] * 8,
        compiler_params=pltpu.CompilerParams(
            collective_id=0, has_side_effects=True, vmem_limit_bytes=VMEM_LIMIT
        ),
    )(*operands)


def per_device(
    latent,
    rotary_key,
    doc_ids,
    queries_content,
    queries_rotary,
    w_key_up,
    w_value_up,
    w_out,
    residual,
    norm_gain,
    routes,
    route_weights,
    w_gate,
    w_up,
    w_down,
    out_gain,
):
    frequency = jnp.asarray(np.tile(ROPE_THETA ** (-2.0 * np.arange(DR // 2) / DR), 4), F32)
    mixed = layer(
        latent,
        rotary_key.T,
        doc_ids.reshape(1, TOK),
        frequency.reshape(1, 128),
        norm_gain.reshape(1, D),
        routes.T,
        route_weights.T,
        out_gain.reshape(1, D),
        queries_content,
        queries_rotary,
        residual,
        w_key_up,
        w_value_up,
        w_out,
        w_gate,
        w_up,
        w_down,
    )
    return mixed


def solution(mesh):
    return jax.shard_map(
        per_device,
        mesh=mesh,
        in_specs=(
            P("sp", None),
            P("sp", None),
            P("sp"),
            P("sp", "tp"),
            P("sp", "tp"),
            P(),
            P(),
            P("tp", None),
            P(("sp", "tp"), None),
            P(),
            P(("sp", "tp"), None),
            P(("sp", "tp"), None),
            P("sp", None, "tp"),
            P("sp", None, "tp"),
            P("sp", "tp", None),
            P(),
        ),
        out_specs=P(("sp", "tp"), None),
        check_vma=False,
    )
```

```python
import jax
import jax.numpy as jnp
import numpy as np
from jax import lax
from jax.experimental import pallas as pl
from jax.experimental.pallas import tpu as pltpu
from jax.sharding import PartitionSpec as P

HEADS = 8
DK = 128
DR = 64
DV = 128
TOPK = 2
REACH = 4
RANK = 256
D = 2048
TOK = 256
ROWS = 128
FFH = 1792
CAP = 8
GROUPS = 4
PEERS = 16
LOCAL_HEADS = 4
CHIPS = 64

ROPE_THETA = 500000.0
RESIDUAL_SCALE = 2.0**0.5
NORM_EPSILON = 1e-05
EXCLUDED = -1e30
LOG2E = 1.4426950408889634
MESH = pl.DeviceIdType.MESH
VMEM_LIMIT = 62_000_000
F32 = jnp.float32
BF16 = jnp.bfloat16


def remote(src, dst, send, recv, chip, core):
    return pltpu.make_async_remote_copy(
        src_ref=src, dst_ref=dst, send_sem=send, recv_sem=recv, device_id=(chip, core), device_id_type=MESH
    )


def layer_norm(values, gain_vec):
    centre = jnp.mean(values, -1, keepdims=True)
    spread = jnp.mean(jnp.square(values - centre), -1, keepdims=True)
    return (values - centre) * lax.rsqrt(spread + NORM_EPSILON) * gain_vec


def layer_kernel(
    latent,
    key_rot,
    doc_row,
    frequency,
    gain,
    routes,
    weights,
    last_gain,
    qc_hbm,
    qr_hbm,
    residual_hbm,
    wk_hbm,
    wv_hbm,
    wo_hbm,
    wg_hbm,
    wu_hbm,
    wd_hbm,
    out,
    qc,
    qr,
    residual,
    aux_out,
    qaux,
    kvl,
    kva,
    wk,
    wv,
    wo,
    peaks,
    scores,
    vals,
    att,
    psend,
    precv,
    nrm,
    wg,
    wu,
    wd,
    obuf,
    xbuf,
    lhs,
    hid,
    ybuf,
    yrecv,
    back,
    wsem,
    ssem,
    rsem,
    fssem,
    frsem,
    psem,
    met,
    dsend,
    drecv,
    fsend,
    frecv,
    ysendsem,
    yrecvsem,
    bsend,
    brecv,
):
    sp = lax.axis_index("sp")
    tp = lax.axis_index("tp")
    other = 1 - tp
    barrier = pltpu.get_barrier_semaphore()

    def signal(semaphore, chip, core):
        pl.semaphore_signal(semaphore, inc=1, device_id=(chip, core), device_id_type=MESH)

    z, y, x = sp // 16, lax.rem(sp // 4, 4), lax.rem(sp, 4)
    y_ring = [z * 16 + lax.rem(y + e, 4) * 4 + x for e in (1, 2, 3)]
    z_ring = [lax.rem(z + e, 4) * 16 + y * 4 + x for e in (1, 2, 3)]
    x_ring = [z * 16 + y * 4 + lax.rem(x + e, 4) for e in (1, 2, 3)]
    near = [lax.rem(sp + e + CHIPS, CHIPS) for e in (1, 2, 3, 4, -1, -2, -3, -4)]
    for chip in near + x_ring + y_ring + z_ring:
        signal(barrier, chip, tp)
    signal(barrier, sp, other)

    half = LOCAL_HEADS * DK
    cols = pl.ds(pl.multiple_of(tp * half, half), half)
    loads = [
        pltpu.make_async_copy(wk_hbm.at[:, cols], wk, wsem.at[0]),
        pltpu.make_async_copy(wv_hbm.at[:, cols], wv, wsem.at[1]),
        pltpu.make_async_copy(wo_hbm, wo, wsem.at[2]),
        pltpu.make_async_copy(wg_hbm.at[0], wg, wsem.at[3]),
        pltpu.make_async_copy(wu_hbm.at[0], wu, wsem.at[4]),
        pltpu.make_async_copy(wd_hbm.at[0], wd, wsem.at[5]),
        pltpu.make_async_copy(qc_hbm, qc, wsem.at[6]),
        pltpu.make_async_copy(qr_hbm, qr, wsem.at[7]),
        pltpu.make_async_copy(residual_hbm, residual, wsem.at[8]),
    ]
    for k in (0, 1, 6, 7, 2, 8):
        loads[k].start()
    mine = pl.ds(pl.multiple_of(tp * ROWS, ROWS), ROWS)
    theirs = pl.ds(pl.multiple_of(other * ROWS, ROWS), ROWS)
    pl.semaphore_wait(barrier, 18)

    def passed_on(d):
        return (tp == 1) & (x + d + 1 >= 4)

    def block_send(i, src, d, chip):
        part = (kvl, kva)[i]
        return remote(src, part.at[d, tp], ssem.at[i, d], rsem.at[i, d], chip, tp)

    def send_own(i, src):
        block_send(i, src.at[mine], REACH - 1, lax.rem(sp + REACH, CHIPS)).start()
        for d in range(REACH - 1):

            @pl.when(jnp.logical_not(passed_on(d)))
            def _(d=d):
                block_send(i, src.at[mine], d, lax.rem(sp + d + 1, CHIPS)).start()

    def pass_on(i):
        for d in range(REACH - 1):

            @pl.when(passed_on(d))
            def _(d=d):
                block_send(i, (kvl, kva)[i].at[REACH - 1, tp], d, x_ring[d]).start()

    send_own(0, latent)

    doc_lane = lax.broadcasted_iota(jnp.int32, (64, TOK), 0)
    marks = (doc_lane == doc_row[...]).astype(F32)
    natural = jnp.transpose(jnp.concatenate([key_rot[...].astype(F32), marks], 0))
    wide = lax.broadcasted_iota(jnp.int32, (TOK, 128), 1)
    content = wide < DR
    low_half = lax.rem(wide, DR) < DR // 2
    position = (sp * TOK + lax.broadcasted_iota(jnp.int32, (TOK, 128), 0)).astype(F32)
    angles = position * frequency[...]
    cos_table = jnp.cos(angles)
    sin_table = jnp.where(low_half, -jnp.sin(angles), jnp.sin(angles))

    def turned(v):
        swapped = jnp.where(low_half, pltpu.roll(v, 128 - DR // 2, 1), pltpu.roll(v, DR // 2, 1))
        return v * cos_table + swapped * sin_table

    aux_out[...] = jnp.where(content, turned(natural), natural).astype(BF16)
    send_own(1, aux_out)
    loads[7].wait()
    fence = jnp.where(wide < DR + 32, (natural - 1.0) * -EXCLUDED, 0.0)
    for pair in range(LOCAL_HEADS // 2):
        two = turned(qr[:, pair * 128 : (pair + 1) * 128].astype(F32))
        first = jnp.where(content, two, fence)
        second = jnp.where(content, pltpu.roll(two, DR, 1), fence)
        qaux[:, pair * 256 : pair * 256 + 128] = first.astype(BF16)
        qaux[:, pair * 256 + 128 : pair * 256 + 256] = second.astype(BF16)

    expert = lax.broadcasted_iota(jnp.int32, (128, ROWS), 0)
    picks = [routes[k : k + 1, :] for k in range(TOPK)]
    member = ((picks[0] == expert) | (picks[1] == expert)).astype(F32).astype(BF16)
    upper = (expert < lax.broadcasted_iota(jnp.int32, (128, ROWS), 1)).astype(F32).astype(BF16)
    before = jnp.dot(member, upper, preferred_element_type=F32)
    slots = []
    for pick in picks:
        rank = jnp.sum(jnp.where(pick == expert, before, 0.0), 0, keepdims=True)
        oz = lax.bitwise_and((pick >> 4) - z, 3)
        oy = lax.bitwise_and((pick >> 2) - y, 3)
        ox = lax.bitwise_and(pick - x, 3)
        place = lax.bitwise_and(oz + oy + ox, 3) * PEERS + oz * 4 + oy
        slots.append(place * CAP + rank.astype(jnp.int32))
    slot_sub = lax.broadcasted_iota(jnp.int32, (CHIPS * CAP, ROWS), 0)
    placing = ((slot_sub == slots[0]) | (slot_sub == slots[1])).astype(F32).astype(BF16)
    table = jnp.where(
        expert == 0,
        slots[0].astype(F32),
        jnp.where(
            expert == 1,
            slots[1].astype(F32),
            jnp.where(expert == 2, weights[0:1, :], jnp.where(expert == 3, weights[1:2, :], 0.0)),
        ),
    )
    by_row = jnp.transpose(table)
    slot_lane = lax.broadcasted_iota(jnp.int32, (ROWS, CHIPS * CAP), 1).astype(F32)
    gathers = [(slot_lane == by_row[:, k : k + 1]).astype(F32).astype(BF16) for k in range(TOPK)]
    shares = [by_row[:, TOPK + k : TOPK + k + 1] for k in range(TOPK)]

    for chip in y_ring:
        signal(met.at[0], chip, tp)
    loads[0].wait()
    loads[1].wait()
    loads[6].wait()
    for load in loads[3:6]:
        load.start()

    rate = (DK + DR) ** (-0.5) * LOG2E
    ones = jnp.ones(((REACH + 1) * TOK, DV), BF16)

    def block(lat, aux, slot):
        span = slice(slot * TOK, (slot + 1) * TOK)
        keys = jnp.dot(lat, wk[...], preferred_element_type=F32).astype(BF16)
        vals[span, :] = jnp.dot(lat, wv[...], preferred_element_type=F32).astype(BF16)
        for h in range(LOCAL_HEADS):
            hs = slice(h * DK, (h + 1) * DK)
            query = jnp.concatenate([qc[:, hs], qaux[:, hs]], 1)
            key = jnp.concatenate([keys[:, hs], aux], 1)
            s = lax.dot_general(query, key, (((1,), (1,)), ((), ())), preferred_element_type=F32)
            if slot == 0:
                r = lax.broadcasted_iota(jnp.int32, (TOK, TOK), 0)
                c = lax.broadcasted_iota(jnp.int32, (TOK, TOK), 1)
                s = jnp.where(c <= r, s, EXCLUDED)
            scores[h, :, span] = s
            peak = jnp.maximum(s[:, :128], s[:, 128:])
            peaks[h] = peak if slot == 0 else jnp.maximum(peaks[h], peak)

    block(latent[...], aux_out[...], 0)
    pl.semaphore_wait(met.at[0], 3)
    for chip in z_ring:
        signal(met.at[1], chip, tp)

    def relays(d, core):
        return [
            remote(part.at[d, core], part.at[d, core], fssem.at[i, d], frsem.at[i, d], sp, other)
            for i, part in enumerate((kvl, kva))
        ]

    def process(d):
        for relay in relays(d, other):
            relay.wait_recv()
        block(kvl[d].reshape(TOK, RANK), kva[d].reshape(TOK, 128), d + 1)

    order = (REACH - 1, 0, 1, 2)
    for n, d in enumerate(order):
        for i, relay in enumerate(relays(d, tp)):
            block_send(i, (kvl, kva)[i].at[d, tp], d, near[3]).wait_recv()
            if n == 0:
                pass_on(i)
            relay.start()
        if n >= 1:
            process(order[n - 1])
    loads[2].wait()
    loads[8].wait()
    process(order[-1])

    for h in range(LOCAL_HEADS):
        hs = slice(h * DV, (h + 1) * DV)
        peak = jnp.max(peaks[h], -1, keepdims=True)
        lifted = jnp.exp2((scores[h] - peak) * rate).astype(BF16)
        made = jnp.dot(lifted, jnp.concatenate([vals[:, hs], ones], 1), preferred_element_type=F32)
        att[:, hs] = (made[:, :DV] / made[:, DV:]).astype(BF16)
    psend[...] = jnp.dot(att[theirs, :], wo[...], preferred_element_type=F32).astype(BF16)
    swap = remote(psend, precv, psem.at[0], psem.at[1], sp, other)
    swap.start()
    own = jnp.dot(att[mine, :], wo[...], preferred_element_type=F32).astype(BF16).astype(F32)
    own = own + RESIDUAL_SCALE * residual[...].astype(F32)
    swap.wait_recv()
    rows_in = layer_norm(own + precv[...].astype(F32), gain[...]).astype(BF16)
    nrm[...] = rows_in

    def there(g, j, sign):
        oz = j // 4
        oy = lax.rem(j, 4)
        ox = lax.rem(g + 8 - oz - oy, 4)
        dz = lax.rem(z + sign * oz + 4, 4)
        dy = lax.rem(y + sign * oy + 4, 4)
        dx = lax.rem(x + sign * ox + 4, 4)
        return dz * 16 + dy * 4 + dx

    pl.semaphore_wait(met.at[1], 3)
    for g in range(GROUPS):
        obuf[g] = (
            jnp.dot(placing[g * ROWS : (g + 1) * ROWS], rows_in, preferred_element_type=F32)
            .astype(BF16)
            .reshape(PEERS, CAP, D)
        )
        first = 1 if g == 0 else 0

        def dispatch(j, carry, g=g):
            remote(obuf.at[g, j], xbuf.at[g, tp, j], dsend.at[g], drecv.at[g], there(g, j, 1), tp).start()
            return carry

        lax.fori_loop(first, PEERS, dispatch, 0)
        if g == 0:
            xbuf[0, tp, 0] = obuf[0, 0]

    def arrived(g):
        first = 1 if isinstance(g, int) and g == 0 else 0
        part = xbuf.at[g, tp, pl.ds(first, PEERS - first)]
        remote(part, part, dsend.at[g], drecv.at[g], sp, other).wait_recv()
        remote(xbuf.at[g, tp], xbuf.at[g, tp], fsend.at[g], frecv.at[g], sp, other).start()

    def swap_of(g):
        return remote(ybuf.at[g, other], yrecv.at[g], ysendsem.at[g], yrecvsem.at[g], sp, other)

    def finish(g):
        swap_of(g).wait_recv()
        ybuf[g, tp] = (ybuf[g, tp].astype(F32) + yrecv[g].astype(F32)).astype(BF16)

        def send_back(j, carry):
            remote(ybuf.at[g, tp, j], back.at[g, j], bsend.at[g], brecv.at[g], there(g, j, -1), tp).start()
            return carry

        lax.fori_loop(jnp.where(g == 0, 1, 0), PEERS, send_back, 0)

    arrived(0)
    for load in loads[3:6]:
        load.wait()

    def group(g, carry):
        part = xbuf.at[g, other]
        remote(part, part, fsend.at[g], frecv.at[g], sp, other).wait_recv()
        lhs[...] = xbuf[g].reshape(TOK, D)
        gate = jnp.dot(lhs[...], wg[...], preferred_element_type=F32)
        up = jnp.dot(lhs[...], wu[...], preferred_element_type=F32)
        hid[...] = (gate / (1.0 + jnp.exp(-gate)) * up).astype(BF16)

        @pl.when(g > 0)
        def _():
            finish(g - 1)

        @pl.when(g + 1 < GROUPS)
        def _():
            arrived(g + 1)

        made = jnp.dot(hid[...], wd[...], preferred_element_type=F32).astype(BF16)
        ybuf[g] = made.reshape(2, PEERS, CAP, D)
        swap_of(g).start()
        return carry

    lax.fori_loop(0, GROUPS, group, 0)
    finish(GROUPS - 1)
    back[0, 0] = ybuf[0, tp, 0]

    combined = RESIDUAL_SCALE * nrm[...].astype(F32)
    picked = [jnp.zeros((ROWS, D), F32) for _ in range(TOPK)]
    for g in range(GROUPS):
        first = 1 if g == 0 else 0
        part = back.at[g, pl.ds(first, PEERS - first)]
        remote(part, part, bsend.at[g], brecv.at[g], sp, other).wait_recv()
        landed = back[g].reshape(ROWS, D)
        for k in range(TOPK):
            picked[k] = picked[k] + jnp.dot(
                gathers[k][:, g * ROWS : (g + 1) * ROWS], landed, preferred_element_type=F32
            )
    for k in range(TOPK):
        combined = combined + picked[k] * shares[k]
    out[...] = layer_norm(combined, last_gain[...]).astype(BF16)

    swap.wait_send()
    for d in range(REACH):
        for i, relay in enumerate(relays(d, tp)):
            block_send(i, (kvl, kva)[i].at[d, tp], d, near[3]).wait_send()
            relay.wait_send()
    for g in range(GROUPS):
        first = 1 if g == 0 else 0
        part = obuf.at[g, pl.ds(first, PEERS - first)]
        remote(part, part, dsend.at[g], drecv.at[g], sp, other).wait_send()
        part = ybuf.at[g, tp, pl.ds(first, PEERS - first)]
        remote(part, part, bsend.at[g], brecv.at[g], sp, other).wait_send()
        remote(xbuf.at[g, tp], xbuf.at[g, tp], fsend.at[g], frecv.at[g], sp, other).wait_send()
        swap_of(g).wait_send()


def in_vmem():
    return pl.BlockSpec(memory_space=pltpu.VMEM)


def in_hbm():
    return pl.BlockSpec(memory_space=pltpu.HBM)


DMA = pltpu.SemaphoreType.DMA


def layer(*operands):
    return pl.pallas_call(
        layer_kernel,
        out_shape=jax.ShapeDtypeStruct((ROWS, D), BF16),
        in_specs=[in_vmem()] * 8 + [in_hbm()] * 9,
        out_specs=in_vmem(),
        scratch_shapes=[
            pltpu.VMEM((TOK, LOCAL_HEADS * DK), BF16),
            pltpu.VMEM((TOK, LOCAL_HEADS * DR), BF16),
            pltpu.VMEM((ROWS, D), BF16),
            pltpu.VMEM((TOK, 128), BF16),
            pltpu.VMEM((TOK, LOCAL_HEADS * 128), BF16),
            pltpu.VMEM((REACH, 2, ROWS, RANK), BF16),
            pltpu.VMEM((REACH, 2, ROWS, 128), BF16),
            pltpu.VMEM((RANK, LOCAL_HEADS * DK), BF16),
            pltpu.VMEM((RANK, LOCAL_HEADS * DV), BF16),
            pltpu.VMEM((LOCAL_HEADS * DV, D), BF16),
            pltpu.VMEM((LOCAL_HEADS, TOK, 128), F32),
            pltpu.VMEM((LOCAL_HEADS, TOK, (REACH + 1) * TOK), F32),
            pltpu.VMEM(((REACH + 1) * TOK, LOCAL_HEADS * DV), BF16),
            pltpu.VMEM((TOK, LOCAL_HEADS * DV), BF16),
            pltpu.VMEM((ROWS, D), BF16),
            pltpu.VMEM((ROWS, D), BF16),
            pltpu.VMEM((ROWS, D), BF16),
            pltpu.VMEM((D, FFH), BF16),
            pltpu.VMEM((D, FFH), BF16),
            pltpu.VMEM((FFH, D), BF16),
            pltpu.VMEM((GROUPS, PEERS, CAP, D), BF16),
            pltpu.VMEM((GROUPS, 2, PEERS, CAP, D), BF16),
            pltpu.VMEM((TOK, D), BF16),
            pltpu.VMEM((TOK, FFH), BF16),
            pltpu.VMEM((GROUPS, 2, PEERS, CAP, D), BF16),
            pltpu.VMEM((GROUPS, PEERS, CAP, D), BF16),
            pltpu.VMEM((GROUPS, PEERS, CAP, D), BF16),
            DMA((9,)),
        ]
        + [DMA((2, REACH))] * 4
        + [DMA((2,)), pltpu.SemaphoreType.REGULAR((2,))]
        + [DMA((GROUPS,))] * 8,
        compiler_params=pltpu.CompilerParams(
            collective_id=0, has_side_effects=True, vmem_limit_bytes=VMEM_LIMIT
        ),
    )(*operands)


def per_device(
    latent,
    rotary_key,
    doc_ids,
    queries_content,
    queries_rotary,
    w_key_up,
    w_value_up,
    w_out,
    residual,
    norm_gain,
    routes,
    route_weights,
    w_gate,
    w_up,
    w_down,
    out_gain,
):
    frequency = jnp.asarray(np.tile(ROPE_THETA ** (-2.0 * np.arange(DR // 2) / DR), 4), F32)
    mixed = layer(
        latent,
        rotary_key.T,
        doc_ids.reshape(1, TOK),
        frequency.reshape(1, 128),
        norm_gain.reshape(1, D),
        routes.T,
        route_weights.T,
        out_gain.reshape(1, D),
        queries_content,
        queries_rotary,
        residual,
        w_key_up,
        w_value_up,
        w_out,
        w_gate,
        w_up,
        w_down,
    )
    return mixed


def solution(mesh):
    return jax.shard_map(
        per_device,
        mesh=mesh,
        in_specs=(
            P("sp", None),
            P("sp", None),
            P("sp"),
            P("sp", "tp"),
            P("sp", "tp"),
            P(),
            P(),
            P("tp", None),
            P(("sp", "tp"), None),
            P(),
            P(("sp", "tp"), None),
            P(("sp", "tp"), None),
            P("sp", None, "tp"),
            P("sp", None, "tp"),
            P("sp", "tp", None),
            P(),
        ),
        out_specs=P(("sp", "tp"), None),
        check_vma=False,
    )
```

```python
import jax
import jax.numpy as jnp
import numpy as np
from jax import lax
from jax.experimental import pallas as pl
from jax.experimental.pallas import tpu as pltpu
from jax.sharding import PartitionSpec as P

HEADS = 8
DK = 128
DR = 64
DV = 128
TOPK = 2
REACH = 4
RANK = 256
D = 2048
TOK = 256
ROWS = 128
FFH = 1792
CAP = 8
GROUPS = 4
PEERS = 16
LOCAL_HEADS = 4
CHIPS = 64

ROPE_THETA = 500000.0
RESIDUAL_SCALE = 2.0**0.5
NORM_EPSILON = 1e-05
EXCLUDED = -1e30
LOG2E = 1.4426950408889634
MESH = pl.DeviceIdType.MESH
VMEM_LIMIT = 62_000_000
F32 = jnp.float32
BF16 = jnp.bfloat16


def remote(src, dst, send, recv, chip, core):
    return pltpu.make_async_remote_copy(
        src_ref=src, dst_ref=dst, send_sem=send, recv_sem=recv, device_id=(chip, core), device_id_type=MESH
    )


def layer_norm(values, gain_vec):
    centre = jnp.mean(values, -1, keepdims=True)
    spread = jnp.mean(jnp.square(values - centre), -1, keepdims=True)
    return (values - centre) * lax.rsqrt(spread + NORM_EPSILON) * gain_vec


def layer_kernel(
    latent_hbm,
    key_rot_hbm,
    doc_row_hbm,
    frequency_hbm,
    gain_hbm,
    routes_hbm,
    weights_hbm,
    last_gain_hbm,
    qc_hbm,
    qr_hbm,
    residual_hbm,
    wk_hbm,
    wv_hbm,
    wo_hbm,
    wg_hbm,
    wu_hbm,
    wd_hbm,
    out,
    latent,
    key_rot,
    doc_row,
    frequency,
    gain,
    routes,
    weights,
    last_gain,
    qc,
    qr,
    residual,
    aux_out,
    qaux,
    kvl,
    kva,
    wk,
    wv,
    wo,
    peaks,
    scores,
    vals,
    att,
    att_in,
    nrm,
    wg,
    wu,
    wd,
    obuf,
    xbuf,
    lhs,
    hid,
    ybuf,
    yrecv,
    back,
    small_sem,
    wsem,
    ssem,
    rsem,
    fssem,
    frsem,
    psem,
    met,
    dsend,
    drecv,
    fsend,
    frecv,
    ysendsem,
    yrecvsem,
    bsend,
    brecv,
):
    sp = lax.axis_index("sp")
    tp = lax.axis_index("tp")
    other = 1 - tp
    barrier = pltpu.get_barrier_semaphore()

    def signal(semaphore, chip, core):
        pl.semaphore_signal(semaphore, inc=1, device_id=(chip, core), device_id_type=MESH)

    z, y, x = sp // 16, lax.rem(sp // 4, 4), lax.rem(sp, 4)
    y_ring = [z * 16 + lax.rem(y + e, 4) * 4 + x for e in (1, 2, 3)]
    z_ring = [lax.rem(z + e, 4) * 16 + y * 4 + x for e in (1, 2, 3)]
    x_ring = [z * 16 + y * 4 + lax.rem(x + e, 4) for e in (1, 2, 3)]
    near = [lax.rem(sp + e + CHIPS, CHIPS) for e in (1, 2, 3, 4, -1, -2, -3, -4)]
    for chip in near + x_ring + y_ring + z_ring:
        signal(barrier, chip, tp)
    signal(barrier, sp, other)

    small = [
        pltpu.make_async_copy(src, dst, small_sem.at[k])
        for k, (src, dst) in enumerate(
            (
                (latent_hbm, latent),
                (key_rot_hbm, key_rot),
                (doc_row_hbm, doc_row),
                (frequency_hbm, frequency),
                (gain_hbm, gain),
                (routes_hbm, routes),
                (weights_hbm, weights),
                (last_gain_hbm, last_gain),
            )
        )
    ]
    for load in small:
        load.start()
    half = LOCAL_HEADS * DK
    cols = pl.ds(pl.multiple_of(tp * half, half), half)
    loads = [
        pltpu.make_async_copy(wk_hbm.at[:, cols], wk, wsem.at[0]),
        pltpu.make_async_copy(wv_hbm.at[:, cols], wv, wsem.at[1]),
        pltpu.make_async_copy(wo_hbm, wo.at[tp], wsem.at[2]),
        pltpu.make_async_copy(wg_hbm.at[0], wg, wsem.at[3]),
        pltpu.make_async_copy(wu_hbm.at[0], wu, wsem.at[4]),
        pltpu.make_async_copy(wd_hbm.at[0], wd, wsem.at[5]),
        pltpu.make_async_copy(qc_hbm, qc, wsem.at[6]),
        pltpu.make_async_copy(qr_hbm, qr, wsem.at[7]),
        pltpu.make_async_copy(residual_hbm, residual, wsem.at[8]),
    ]
    for k in (0, 1, 6, 7, 2, 8):
        loads[k].start()
    mine = pl.ds(pl.multiple_of(tp * ROWS, ROWS), ROWS)
    theirs = pl.ds(pl.multiple_of(other * ROWS, ROWS), ROWS)
    for load in small:
        load.wait()
    pl.semaphore_wait(barrier, 18)

    def passed_on(d):
        return (tp == 1) & (x + d + 1 >= 4)

    def block_send(i, src, d, chip):
        part = (kvl, kva)[i]
        return remote(src, part.at[d, tp], ssem.at[i, d], rsem.at[i, d], chip, tp)

    def send_own(i, src):
        block_send(i, src.at[mine], REACH - 1, lax.rem(sp + REACH, CHIPS)).start()
        for d in (2, 1, 0):

            @pl.when(jnp.logical_not(passed_on(d)))
            def _(d=d):
                block_send(i, src.at[mine], d, lax.rem(sp + d + 1, CHIPS)).start()

    def pass_on(i):
        for d in (2, 1, 0):

            @pl.when(passed_on(d))
            def _(d=d):
                block_send(i, (kvl, kva)[i].at[REACH - 1, tp], d, x_ring[d]).start()

    send_own(0, latent)
    loads[2].wait()
    share = remote(wo.at[tp], wo.at[tp], psem.at[2], psem.at[3], sp, other)
    share.start()

    doc_lane = lax.broadcasted_iota(jnp.int32, (64, TOK), 0)
    marks = (doc_lane == doc_row[...]).astype(F32)
    natural = jnp.transpose(jnp.concatenate([key_rot[...].astype(F32), marks], 0))
    wide = lax.broadcasted_iota(jnp.int32, (TOK, 128), 1)
    content = wide < DR
    low_half = lax.rem(wide, DR) < DR // 2
    position = (sp * TOK + lax.broadcasted_iota(jnp.int32, (TOK, 128), 0)).astype(F32)
    angles = position * frequency[...]
    cos_table = jnp.cos(angles)
    sin_table = jnp.where(low_half, -jnp.sin(angles), jnp.sin(angles))

    def turned(v):
        swapped = jnp.where(low_half, pltpu.roll(v, 128 - DR // 2, 1), pltpu.roll(v, DR // 2, 1))
        return v * cos_table + swapped * sin_table

    aux_out[...] = jnp.where(content, turned(natural), natural).astype(BF16)
    send_own(1, aux_out)
    loads[7].wait()
    fence = jnp.where(wide < DR + 32, (natural - 1.0) * -EXCLUDED, 0.0)
    for pair in range(LOCAL_HEADS // 2):
        two = turned(qr[:, pair * 128 : (pair + 1) * 128].astype(F32))
        first = jnp.where(content, two, fence)
        second = jnp.where(content, pltpu.roll(two, DR, 1), fence)
        qaux[:, pair * 256 : pair * 256 + 128] = first.astype(BF16)
        qaux[:, pair * 256 + 128 : pair * 256 + 256] = second.astype(BF16)

    expert = lax.broadcasted_iota(jnp.int32, (128, ROWS), 0)
    picks = [routes[k : k + 1, :] for k in range(TOPK)]
    member = ((picks[0] == expert) | (picks[1] == expert)).astype(F32).astype(BF16)
    upper = (expert < lax.broadcasted_iota(jnp.int32, (128, ROWS), 1)).astype(F32).astype(BF16)
    before = jnp.dot(member, upper, preferred_element_type=F32)
    slots = []
    for pick in picks:
        rank = jnp.sum(jnp.where(pick == expert, before, 0.0), 0, keepdims=True)
        oz = lax.bitwise_and((pick >> 4) - z, 3)
        oy = lax.bitwise_and((pick >> 2) - y, 3)
        ox = lax.bitwise_and(pick - x, 3)
        place = lax.bitwise_and(oz + oy + ox, 3) * PEERS + oz * 4 + oy
        slots.append(place * CAP + rank.astype(jnp.int32))
    slot_sub = lax.broadcasted_iota(jnp.int32, (CHIPS * CAP, ROWS), 0)
    placing = ((slot_sub == slots[0]) | (slot_sub == slots[1])).astype(F32).astype(BF16)
    table = jnp.where(
        expert == 0,
        slots[0].astype(F32),
        jnp.where(
            expert == 1,
            slots[1].astype(F32),
            jnp.where(expert == 2, weights[0:1, :], jnp.where(expert == 3, weights[1:2, :], 0.0)),
        ),
    )
    by_row = jnp.transpose(table)
    slot_lane = lax.broadcasted_iota(jnp.int32, (ROWS, CHIPS * CAP), 1).astype(F32)
    gathers = [(slot_lane == by_row[:, k : k + 1]).astype(F32).astype(BF16) for k in range(TOPK)]
    shares = [by_row[:, TOPK + k : TOPK + k + 1] for k in range(TOPK)]

    for chip in y_ring:
        signal(met.at[0], chip, tp)
    loads[0].wait()
    loads[1].wait()
    loads[6].wait()
    for load in loads[3:6]:
        load.start()

    rate = (DK + DR) ** (-0.5) * LOG2E
    ones = jnp.ones(((REACH + 1) * TOK, DV), BF16)

    def block(lat, aux, slot):
        span = slice(slot * TOK, (slot + 1) * TOK)
        keys = jnp.dot(lat, wk[...], preferred_element_type=F32).astype(BF16)
        vals[span, :] = jnp.dot(lat, wv[...], preferred_element_type=F32).astype(BF16)
        for h in range(LOCAL_HEADS):
            hs = slice(h * DK, (h + 1) * DK)
            query = jnp.concatenate([qc[:, hs], qaux[:, hs]], 1)
            key = jnp.concatenate([keys[:, hs], aux], 1)
            s = lax.dot_general(query, key, (((1,), (1,)), ((), ())), preferred_element_type=F32)
            if slot == 0:
                r = lax.broadcasted_iota(jnp.int32, (TOK, TOK), 0)
                c = lax.broadcasted_iota(jnp.int32, (TOK, TOK), 1)
                s = jnp.where(c <= r, s, EXCLUDED)
            scores[h, :, span] = s
            peak = jnp.maximum(s[:, :128], s[:, 128:])
            peaks[h] = peak if slot == 0 else jnp.maximum(peaks[h], peak)

    block(latent[...], aux_out[...], 0)
    pl.semaphore_wait(met.at[0], 3)
    for chip in z_ring:
        signal(met.at[1], chip, tp)

    def relays(d, core):
        return [
            remote(part.at[d, core], part.at[d, core], fssem.at[i, d], frsem.at[i, d], sp, other)
            for i, part in enumerate((kvl, kva))
        ]

    def process(d):
        for relay in relays(d, other):
            relay.wait_recv()
        block(kvl[d].reshape(TOK, RANK), kva[d].reshape(TOK, 128), d + 1)

    order = (REACH - 1, 2, 1, 0)
    for n, d in enumerate(order):
        for i, relay in enumerate(relays(d, tp)):
            block_send(i, (kvl, kva)[i].at[d, tp], d, near[3]).wait_recv()
            if n == 0:
                pass_on(i)
            relay.start()
        if n >= 1:
            process(order[n - 1])
    loads[8].wait()
    process(order[-1])

    for h in range(LOCAL_HEADS):
        hs = slice(h * DV, (h + 1) * DV)
        peak = jnp.max(peaks[h], -1, keepdims=True)
        lifted = jnp.exp2((scores[h] - peak) * rate).astype(BF16)
        made = jnp.dot(lifted, jnp.concatenate([vals[:, hs], ones], 1), preferred_element_type=F32)
        att[:, hs] = (made[:, :DV] / made[:, DV:]).astype(BF16)
    swap = remote(att.at[theirs], att_in, psem.at[0], psem.at[1], sp, other)
    swap.start()
    own = jnp.dot(att[mine, :], wo[tp], preferred_element_type=F32).astype(BF16).astype(F32)
    own = own + RESIDUAL_SCALE * residual[...].astype(F32)
    remote(wo.at[other], wo.at[other], psem.at[2], psem.at[3], sp, other).wait_recv()
    swap.wait_recv()
    rest = jnp.dot(att_in[...], wo[other], preferred_element_type=F32).astype(BF16).astype(F32)
    rows_in = layer_norm(own + rest, gain[...]).astype(BF16)
    nrm[...] = rows_in

    def there(g, j, sign):
        oz = j // 4
        oy = lax.rem(j, 4)
        ox = lax.rem(g + 8 - oz - oy, 4)
        dz = lax.rem(z + sign * oz + 4, 4)
        dy = lax.rem(y + sign * oy + 4, 4)
        dx = lax.rem(x + sign * ox + 4, 4)
        return dz * 16 + dy * 4 + dx

    pl.semaphore_wait(met.at[1], 3)
    for g in range(GROUPS):
        obuf[g] = (
            jnp.dot(placing[g * ROWS : (g + 1) * ROWS], rows_in, preferred_element_type=F32)
            .astype(BF16)
            .reshape(PEERS, CAP, D)
        )
        first = 1 if g == 0 else 0

        def dispatch(j, carry, g=g):
            j = jnp.where(tp == 1, PEERS - 1 + (1 if g == 0 else 0) - j, j)
            remote(obuf.at[g, j], xbuf.at[g, tp, j], dsend.at[g], drecv.at[g], there(g, j, 1), tp).start()
            return carry

        lax.fori_loop(first, PEERS, dispatch, 0)
        if g == 0:
            xbuf[0, tp, 0] = obuf[0, 0]

    def arrived(g):
        first = 1 if isinstance(g, int) and g == 0 else 0
        part = xbuf.at[g, tp, pl.ds(first, PEERS - first)]
        remote(part, part, dsend.at[g], drecv.at[g], sp, other).wait_recv()
        remote(xbuf.at[g, tp], xbuf.at[g, tp], fsend.at[g], frecv.at[g], sp, other).start()

    def swap_of(g):
        return remote(ybuf.at[g, other], yrecv.at[g], ysendsem.at[g], yrecvsem.at[g], sp, other)

    def finish(g):
        swap_of(g).wait_recv()
        ybuf[g, tp] = (ybuf[g, tp].astype(F32) + yrecv[g].astype(F32)).astype(BF16)

        def send_back(j, carry):
            j = jnp.where(tp == 1, PEERS - 1 + jnp.where(g == 0, 1, 0) - j, j)
            remote(ybuf.at[g, tp, j], back.at[g, j], bsend.at[g], brecv.at[g], there(g, j, -1), tp).start()
            return carry

        lax.fori_loop(jnp.where(g == 0, 1, 0), PEERS, send_back, 0)

    arrived(0)
    for load in loads[3:6]:
        load.wait()

    def group(g, carry):
        part = xbuf.at[g, other]
        remote(part, part, fsend.at[g], frecv.at[g], sp, other).wait_recv()
        lhs[...] = xbuf[g].reshape(TOK, D)
        gate = jnp.dot(lhs[...], wg[...], preferred_element_type=F32)
        up = jnp.dot(lhs[...], wu[...], preferred_element_type=F32)
        hid[...] = (gate / (1.0 + jnp.exp(-gate)) * up).astype(BF16)

        @pl.when(g > 0)
        def _():
            finish(g - 1)

        @pl.when(g + 1 < GROUPS)
        def _():
            arrived(g + 1)

        made = jnp.dot(hid[...], wd[...], preferred_element_type=F32).astype(BF16)
        ybuf[g] = made.reshape(2, PEERS, CAP, D)
        swap_of(g).start()
        return carry

    lax.fori_loop(0, GROUPS, group, 0)
    finish(GROUPS - 1)
    back[0, 0] = ybuf[0, tp, 0]

    combined = RESIDUAL_SCALE * nrm[...].astype(F32)
    picked = [jnp.zeros((ROWS, D), F32) for _ in range(TOPK)]
    for g in range(GROUPS):
        first = 1 if g == 0 else 0
        part = back.at[g, pl.ds(first, PEERS - first)]
        remote(part, part, bsend.at[g], brecv.at[g], sp, other).wait_recv()
        landed = back[g].reshape(ROWS, D)
        for k in range(TOPK):
            picked[k] = picked[k] + jnp.dot(
                gathers[k][:, g * ROWS : (g + 1) * ROWS], landed, preferred_element_type=F32
            )
    for k in range(TOPK):
        combined = combined + picked[k] * shares[k]
    out[...] = layer_norm(combined, last_gain[...]).astype(BF16)

    swap.wait_send()
    share.wait_send()
    for d in range(REACH):
        for i, relay in enumerate(relays(d, tp)):
            block_send(i, (kvl, kva)[i].at[d, tp], d, near[3]).wait_send()
            relay.wait_send()
    for g in range(GROUPS):
        first = 1 if g == 0 else 0
        part = obuf.at[g, pl.ds(first, PEERS - first)]
        remote(part, part, dsend.at[g], drecv.at[g], sp, other).wait_send()
        part = ybuf.at[g, tp, pl.ds(first, PEERS - first)]
        remote(part, part, bsend.at[g], brecv.at[g], sp, other).wait_send()
        remote(xbuf.at[g, tp], xbuf.at[g, tp], fsend.at[g], frecv.at[g], sp, other).wait_send()
        swap_of(g).wait_send()


def in_vmem():
    return pl.BlockSpec(memory_space=pltpu.VMEM)


def in_hbm():
    return pl.BlockSpec(memory_space=pltpu.HBM)


DMA = pltpu.SemaphoreType.DMA


def layer(*operands):
    return pl.pallas_call(
        layer_kernel,
        out_shape=jax.ShapeDtypeStruct((ROWS, D), BF16),
        in_specs=[in_hbm()] * 17,
        out_specs=in_vmem(),
        scratch_shapes=[
            pltpu.VMEM((TOK, RANK), BF16),
            pltpu.VMEM((DR, TOK), BF16),
            pltpu.VMEM((1, TOK), jnp.int32),
            pltpu.VMEM((1, 128), F32),
            pltpu.VMEM((1, D), F32),
            pltpu.VMEM((TOPK, ROWS), jnp.int32),
            pltpu.VMEM((TOPK, ROWS), F32),
            pltpu.VMEM((1, D), F32),
            pltpu.VMEM((TOK, LOCAL_HEADS * DK), BF16),
            pltpu.VMEM((TOK, LOCAL_HEADS * DR), BF16),
            pltpu.VMEM((ROWS, D), BF16),
            pltpu.VMEM((TOK, 128), BF16),
            pltpu.VMEM((TOK, LOCAL_HEADS * 128), BF16),
            pltpu.VMEM((REACH, 2, ROWS, RANK), BF16),
            pltpu.VMEM((REACH, 2, ROWS, 128), BF16),
            pltpu.VMEM((RANK, LOCAL_HEADS * DK), BF16),
            pltpu.VMEM((RANK, LOCAL_HEADS * DV), BF16),
            pltpu.VMEM((2, LOCAL_HEADS * DV, D), BF16),
            pltpu.VMEM((LOCAL_HEADS, TOK, 128), F32),
            pltpu.VMEM((LOCAL_HEADS, TOK, (REACH + 1) * TOK), F32),
            pltpu.VMEM(((REACH + 1) * TOK, LOCAL_HEADS * DV), BF16),
            pltpu.VMEM((TOK, LOCAL_HEADS * DV), BF16),
            pltpu.VMEM((ROWS, LOCAL_HEADS * DV), BF16),
            pltpu.VMEM((ROWS, D), BF16),
            pltpu.VMEM((D, FFH), BF16),
            pltpu.VMEM((D, FFH), BF16),
            pltpu.VMEM((FFH, D), BF16),
            pltpu.VMEM((GROUPS, PEERS, CAP, D), BF16),
            pltpu.VMEM((GROUPS, 2, PEERS, CAP, D), BF16),
            pltpu.VMEM((TOK, D), BF16),
            pltpu.VMEM((TOK, FFH), BF16),
            pltpu.VMEM((GROUPS, 2, PEERS, CAP, D), BF16),
            pltpu.VMEM((GROUPS, PEERS, CAP, D), BF16),
            pltpu.VMEM((GROUPS, PEERS, CAP, D), BF16),
            DMA((8,)),
            DMA((9,)),
        ]
        + [DMA((2, REACH))] * 4
        + [DMA((4,)), pltpu.SemaphoreType.REGULAR((2,))]
        + [DMA((GROUPS,))] * 8,
        compiler_params=pltpu.CompilerParams(
            collective_id=0, has_side_effects=True, vmem_limit_bytes=VMEM_LIMIT
        ),
    )(*operands)


def per_device(
    latent,
    rotary_key,
    doc_ids,
    queries_content,
    queries_rotary,
    w_key_up,
    w_value_up,
    w_out,
    residual,
    norm_gain,
    routes,
    route_weights,
    w_gate,
    w_up,
    w_down,
    out_gain,
):
    frequency = jnp.asarray(np.tile(ROPE_THETA ** (-2.0 * np.arange(DR // 2) / DR), 4), F32)
    mixed = layer(
        latent,
        rotary_key.T,
        doc_ids.reshape(1, TOK),
        frequency.reshape(1, 128),
        norm_gain.reshape(1, D),
        routes.T,
        route_weights.T,
        out_gain.reshape(1, D),
        queries_content,
        queries_rotary,
        residual,
        w_key_up,
        w_value_up,
        w_out,
        w_gate,
        w_up,
        w_down,
    )
    return mixed


def solution(mesh):
    return jax.shard_map(
        per_device,
        mesh=mesh,
        in_specs=(
            P("sp", None),
            P("sp", None),
            P("sp"),
            P("sp", "tp"),
            P("sp", "tp"),
            P(),
            P(),
            P("tp", None),
            P(("sp", "tp"), None),
            P(),
            P(("sp", "tp"), None),
            P(("sp", "tp"), None),
            P("sp", None, "tp"),
            P("sp", None, "tp"),
            P("sp", "tp", None),
            P(),
        ),
        out_specs=P(("sp", "tp"), None),
        check_vma=False,
    )
```

```python
import jax
import jax.numpy as jnp
import numpy as np
from jax import lax
from jax.experimental import pallas as pl
from jax.experimental.pallas import tpu as pltpu
from jax.sharding import PartitionSpec as P

HEADS = 8
DK = 128
DR = 64
DV = 128
TOPK = 2
REACH = 4
RANK = 256
D = 2048
TOK = 256
ROWS = 128
FFH = 1792
CAP = 8
GROUPS = 4
PEERS = 16
LOCAL_HEADS = 4
CHIPS = 64

ROPE_THETA = 500000.0
RESIDUAL_SCALE = 2.0**0.5
NORM_EPSILON = 1e-05
EXCLUDED = -1e30
LOG2E = 1.4426950408889634
MESH = pl.DeviceIdType.MESH
VMEM_LIMIT = 62_000_000
F32 = jnp.float32
BF16 = jnp.bfloat16


def remote(src, dst, send, recv, chip, core):
    return pltpu.make_async_remote_copy(
        src_ref=src, dst_ref=dst, send_sem=send, recv_sem=recv, device_id=(chip, core), device_id_type=MESH
    )


def layer_norm(values, gain_vec):
    centre = jnp.mean(values, -1, keepdims=True)
    spread = jnp.mean(jnp.square(values - centre), -1, keepdims=True)
    return (values - centre) * lax.rsqrt(spread + NORM_EPSILON) * gain_vec


def layer_kernel(
    latent_hbm,
    key_rot_hbm,
    doc_row_hbm,
    frequency_hbm,
    gain_hbm,
    routes_hbm,
    weights_hbm,
    last_gain_hbm,
    qc_hbm,
    qr_hbm,
    residual_hbm,
    wk_hbm,
    wv_hbm,
    wo_hbm,
    wg_hbm,
    wu_hbm,
    wd_hbm,
    out,
    latent,
    key_rot,
    doc_row,
    frequency,
    gain,
    routes,
    weights,
    last_gain,
    qc,
    qr,
    residual,
    aux_out,
    qaux,
    kvl,
    kva,
    wk,
    wv,
    wo,
    peaks,
    scores,
    vals,
    att,
    att_in,
    nrm,
    wg,
    wu,
    wd,
    obuf,
    xbuf,
    lhs,
    hid,
    ybuf,
    yrecv,
    back,
    small_sem,
    wsem,
    ssem,
    rsem,
    fssem,
    frsem,
    psem,
    met,
    dsend,
    drecv,
    fsend,
    frecv,
    ysendsem,
    yrecvsem,
    bsend,
    brecv,
):
    sp = lax.axis_index("sp")
    tp = lax.axis_index("tp")
    other = 1 - tp
    barrier = pltpu.get_barrier_semaphore()

    def signal(semaphore, chip, core):
        pl.semaphore_signal(semaphore, inc=1, device_id=(chip, core), device_id_type=MESH)

    z, y, x = sp // 16, lax.rem(sp // 4, 4), lax.rem(sp, 4)
    y_ring = [z * 16 + lax.rem(y + e, 4) * 4 + x for e in (1, 2, 3)]
    z_ring = [lax.rem(z + e, 4) * 16 + y * 4 + x for e in (1, 2, 3)]
    x_ring = [z * 16 + y * 4 + lax.rem(x + e, 4) for e in (1, 2, 3)]
    near = [lax.rem(sp + e + CHIPS, CHIPS) for e in (1, 2, 3, 4, -1, -2, -3, -4)]
    for chip in near + x_ring + y_ring + z_ring:
        signal(barrier, chip, tp)
    signal(barrier, sp, other)

    small = [
        pltpu.make_async_copy(src, dst, small_sem.at[k])
        for k, (src, dst) in enumerate(
            (
                (latent_hbm, latent),
                (key_rot_hbm, key_rot),
                (doc_row_hbm, doc_row),
                (frequency_hbm, frequency),
                (gain_hbm, gain),
                (routes_hbm, routes),
                (weights_hbm, weights),
                (last_gain_hbm, last_gain),
            )
        )
    ]
    for load in small:
        load.start()
    half = LOCAL_HEADS * DK
    cols = pl.ds(pl.multiple_of(tp * half, half), half)
    loads = [
        pltpu.make_async_copy(wk_hbm.at[:, cols], wk, wsem.at[0]),
        pltpu.make_async_copy(wv_hbm.at[:, cols], wv, wsem.at[1]),
        pltpu.make_async_copy(wo_hbm, wo.at[tp], wsem.at[2]),
        pltpu.make_async_copy(wg_hbm.at[0], wg, wsem.at[3]),
        pltpu.make_async_copy(wu_hbm.at[0], wu, wsem.at[4]),
        pltpu.make_async_copy(wd_hbm.at[0], wd, wsem.at[5]),
        pltpu.make_async_copy(qc_hbm, qc, wsem.at[6]),
        pltpu.make_async_copy(qr_hbm, qr, wsem.at[7]),
        pltpu.make_async_copy(residual_hbm, residual, wsem.at[8]),
    ]
    for k in (0, 1, 6, 7, 2, 8):
        loads[k].start()
    mine = pl.ds(pl.multiple_of(tp * ROWS, ROWS), ROWS)
    theirs = pl.ds(pl.multiple_of(other * ROWS, ROWS), ROWS)
    for load in small:
        load.wait()
    pl.semaphore_wait(barrier, 18)

    def passed_on(d):
        return (tp == 1) & (x + d + 1 >= 4)

    def block_send(i, src, d, chip):
        part = (kvl, kva)[i]
        return remote(src, part.at[d, tp], ssem.at[i, d], rsem.at[i, d], chip, tp)

    def send_own(i, src):
        block_send(i, src.at[mine], REACH - 1, lax.rem(sp + REACH, CHIPS)).start()
        for d in (2, 1, 0):

            @pl.when(jnp.logical_not(passed_on(d)))
            def _(d=d):
                block_send(i, src.at[mine], d, lax.rem(sp + d + 1, CHIPS)).start()

    def pass_on(i):
        for d in (2, 1, 0):

            @pl.when(passed_on(d))
            def _(d=d):
                block_send(i, (kvl, kva)[i].at[REACH - 1, tp], d, x_ring[d]).start()

    send_own(0, latent)
    loads[2].wait()
    share = remote(wo.at[tp], wo.at[tp], psem.at[2], psem.at[3], sp, other)
    share.start()

    doc_lane = lax.broadcasted_iota(jnp.int32, (64, TOK), 0)
    marks = (doc_lane == doc_row[...]).astype(F32)
    natural = jnp.transpose(jnp.concatenate([key_rot[...].astype(F32), marks], 0))
    wide = lax.broadcasted_iota(jnp.int32, (TOK, 128), 1)
    content = wide < DR
    low_half = lax.rem(wide, DR) < DR // 2
    position = (sp * TOK + lax.broadcasted_iota(jnp.int32, (TOK, 128), 0)).astype(F32)
    angles = position * frequency[...]
    cos_table = jnp.cos(angles)
    sin_table = jnp.where(low_half, -jnp.sin(angles), jnp.sin(angles))

    def turned(v):
        swapped = jnp.where(low_half, pltpu.roll(v, 128 - DR // 2, 1), pltpu.roll(v, DR // 2, 1))
        return v * cos_table + swapped * sin_table

    aux_out[...] = jnp.where(content, turned(natural), natural).astype(BF16)
    send_own(1, aux_out)
    loads[7].wait()
    fence = jnp.where(wide < DR + 32, (natural - 1.0) * -EXCLUDED, 0.0)
    for pair in range(LOCAL_HEADS // 2):
        two = turned(qr[:, pair * 128 : (pair + 1) * 128].astype(F32))
        first = jnp.where(content, two, fence)
        second = jnp.where(content, pltpu.roll(two, DR, 1), fence)
        qaux[:, pair * 256 : pair * 256 + 128] = first.astype(BF16)
        qaux[:, pair * 256 + 128 : pair * 256 + 256] = second.astype(BF16)

    expert = lax.broadcasted_iota(jnp.int32, (128, ROWS), 0)
    picks = [routes[k : k + 1, :] for k in range(TOPK)]
    member = ((picks[0] == expert) | (picks[1] == expert)).astype(F32).astype(BF16)
    upper = (expert < lax.broadcasted_iota(jnp.int32, (128, ROWS), 1)).astype(F32).astype(BF16)
    before = jnp.dot(member, upper, preferred_element_type=F32)
    slots = []
    for pick in picks:
        rank = jnp.sum(jnp.where(pick == expert, before, 0.0), 0, keepdims=True)
        oz = lax.bitwise_and((pick >> 4) - z, 3)
        oy = lax.bitwise_and((pick >> 2) - y, 3)
        ox = lax.bitwise_and(pick - x, 3)
        place = lax.bitwise_and(oz + oy + ox, 3) * PEERS + oz * 4 + oy
        slots.append(place * CAP + rank.astype(jnp.int32))
    slot_sub = lax.broadcasted_iota(jnp.int32, (CHIPS * CAP, ROWS), 0)
    placing = ((slot_sub == slots[0]) | (slot_sub == slots[1])).astype(F32).astype(BF16)
    table = jnp.where(
        expert == 0,
        slots[0].astype(F32),
        jnp.where(
            expert == 1,
            slots[1].astype(F32),
            jnp.where(expert == 2, weights[0:1, :], jnp.where(expert == 3, weights[1:2, :], 0.0)),
        ),
    )
    by_row = jnp.transpose(table)
    slot_lane = lax.broadcasted_iota(jnp.int32, (ROWS, CHIPS * CAP), 1).astype(F32)
    gathers = [(slot_lane == by_row[:, k : k + 1]).astype(F32).astype(BF16) for k in range(TOPK)]
    shares = [by_row[:, TOPK + k : TOPK + k + 1] for k in range(TOPK)]

    for chip in y_ring:
        signal(met.at[0], chip, tp)
    loads[0].wait()
    loads[1].wait()
    loads[6].wait()
    for load in loads[3:6]:
        load.start()

    rate = (DK + DR) ** (-0.5) * LOG2E
    ones = jnp.ones(((REACH + 1) * TOK, DV), BF16)

    def block(lat, aux, slot):
        span = slice(slot * TOK, (slot + 1) * TOK)
        keys = jnp.dot(lat, wk[...], preferred_element_type=F32).astype(BF16)
        vals[span, :] = jnp.dot(lat, wv[...], preferred_element_type=F32).astype(BF16)
        for h in range(LOCAL_HEADS):
            hs = slice(h * DK, (h + 1) * DK)
            query = jnp.concatenate([qc[:, hs], qaux[:, hs]], 1)
            key = jnp.concatenate([keys[:, hs], aux], 1)
            s = lax.dot_general(query, key, (((1,), (1,)), ((), ())), preferred_element_type=F32)
            if slot == 0:
                r = lax.broadcasted_iota(jnp.int32, (TOK, TOK), 0)
                c = lax.broadcasted_iota(jnp.int32, (TOK, TOK), 1)
                s = jnp.where(c <= r, s, EXCLUDED)
            scores[h, :, span] = s
            peak = jnp.maximum(s[:, :128], s[:, 128:])
            peaks[h] = peak if slot == 0 else jnp.maximum(peaks[h], peak)

    block(latent[...], aux_out[...], 0)
    pl.semaphore_wait(met.at[0], 3)
    for chip in z_ring:
        signal(met.at[1], chip, tp)

    def relays(d, core):
        return [
            remote(part.at[d, core], part.at[d, core], fssem.at[i, d], frsem.at[i, d], sp, other)
            for i, part in enumerate((kvl, kva))
        ]

    def process(d):
        for relay in relays(d, other):
            relay.wait_recv()
        block(kvl[d].reshape(TOK, RANK), kva[d].reshape(TOK, 128), d + 1)

    order = (REACH - 1, 2, 1, 0)
    for n, d in enumerate(order):
        for i, relay in enumerate(relays(d, tp)):
            block_send(i, (kvl, kva)[i].at[d, tp], d, near[3]).wait_recv()
            if n == 0:
                pass_on(i)
            relay.start()
        if n >= 1:
            process(order[n - 1])
    loads[8].wait()
    process(order[-1])

    for h in range(LOCAL_HEADS):
        hs = slice(h * DV, (h + 1) * DV)
        peak = jnp.max(peaks[h], -1, keepdims=True)
        lifted = jnp.exp2((scores[h] - peak) * rate).astype(BF16)
        made = jnp.dot(lifted, jnp.concatenate([vals[:, hs], ones], 1), preferred_element_type=F32)
        att[:, hs] = (made[:, :DV] / made[:, DV:]).astype(BF16)
    swap = remote(att.at[theirs], att_in, psem.at[0], psem.at[1], sp, other)
    swap.start()
    own = jnp.dot(att[mine, :], wo[tp], preferred_element_type=F32).astype(BF16).astype(F32)
    own = own + RESIDUAL_SCALE * residual[...].astype(F32)
    remote(wo.at[other], wo.at[other], psem.at[2], psem.at[3], sp, other).wait_recv()
    swap.wait_recv()
    rest = jnp.dot(att_in[...], wo[other], preferred_element_type=F32).astype(BF16).astype(F32)
    rows_in = layer_norm(own + rest, gain[...]).astype(BF16)
    nrm[...] = rows_in

    def there(g, j, sign):
        oz = j // 4
        oy = lax.rem(j, 4)
        ox = lax.rem(g + 8 - oz - oy, 4)
        dz = lax.rem(z + sign * oz + 4, 4)
        dy = lax.rem(y + sign * oy + 4, 4)
        dx = lax.rem(x + sign * ox + 4, 4)
        return dz * 16 + dy * 4 + dx

    pl.semaphore_wait(met.at[1], 3)
    for g in range(GROUPS):
        obuf[g] = (
            jnp.dot(placing[g * ROWS : (g + 1) * ROWS], rows_in, preferred_element_type=F32)
            .astype(BF16)
            .reshape(PEERS, CAP, D)
        )
        first = 1 if g == 0 else 0

        def dispatch(j, carry, g=g):
            j = jnp.where(tp == 1, PEERS - 1 + (1 if g == 0 else 0) - j, j)
            remote(obuf.at[g, j], xbuf.at[g, tp, j], dsend.at[g], drecv.at[g], there(g, j, 1), tp).start()
            return carry

        lax.fori_loop(first, PEERS, dispatch, 0)
        if g == 0:
            xbuf[0, tp, 0] = obuf[0, 0]

    def arrived(g):
        first = 1 if isinstance(g, int) and g == 0 else 0
        part = xbuf.at[g, tp, pl.ds(first, PEERS - first)]
        remote(part, part, dsend.at[g], drecv.at[g], sp, other).wait_recv()
        remote(xbuf.at[g, tp], xbuf.at[g, tp], fsend.at[g], frecv.at[g], sp, other).start()

    def swap_of(g):
        return remote(ybuf.at[g, other], yrecv.at[g], ysendsem.at[g], yrecvsem.at[g], sp, other)

    def finish(g):
        swap_of(g).wait_recv()
        ybuf[g, tp] = (ybuf[g, tp].astype(F32) + yrecv[g].astype(F32)).astype(BF16)

        def send_back(j, carry):
            j = jnp.where(tp == 1, PEERS - 1 + jnp.where(g == 0, 1, 0) - j, j)
            remote(ybuf.at[g, tp, j], back.at[g, j], bsend.at[g], brecv.at[g], there(g, j, -1), tp).start()
            return carry

        lax.fori_loop(jnp.where(g == 0, 1, 0), PEERS, send_back, 0)

    arrived(0)
    for load in loads[3:6]:
        load.wait()

    def group(g, carry):
        part = xbuf.at[g, other]
        remote(part, part, fsend.at[g], frecv.at[g], sp, other).wait_recv()
        lhs[...] = xbuf[g].reshape(TOK, D)
        gate = jnp.dot(lhs[...], wg[...], preferred_element_type=F32)
        up = jnp.dot(lhs[...], wu[...], preferred_element_type=F32)
        hid[...] = (gate / (1.0 + jnp.exp(-gate)) * up).astype(BF16)

        @pl.when(g + 1 < GROUPS)
        def _():
            arrived(g + 1)

        @pl.when(g > 0)
        def _():
            finish(g - 1)

        made = jnp.dot(hid[...], wd[...], preferred_element_type=F32).astype(BF16)
        ybuf[g] = made.reshape(2, PEERS, CAP, D)
        swap_of(g).start()
        return carry

    lax.fori_loop(0, GROUPS, group, 0)
    finish(GROUPS - 1)
    back[0, 0] = ybuf[0, tp, 0]

    combined = RESIDUAL_SCALE * nrm[...].astype(F32)
    picked = [jnp.zeros((ROWS, D), F32) for _ in range(TOPK)]
    for g in range(GROUPS):
        first = 1 if g == 0 else 0
        part = back.at[g, pl.ds(first, PEERS - first)]
        remote(part, part, bsend.at[g], brecv.at[g], sp, other).wait_recv()
        landed = back[g].reshape(ROWS, D)
        for k in range(TOPK):
            picked[k] = picked[k] + jnp.dot(
                gathers[k][:, g * ROWS : (g + 1) * ROWS], landed, preferred_element_type=F32
            )
    for k in range(TOPK):
        combined = combined + picked[k] * shares[k]
    out[...] = layer_norm(combined, last_gain[...]).astype(BF16)

    swap.wait_send()
    share.wait_send()
    for d in range(REACH):
        for i, relay in enumerate(relays(d, tp)):
            block_send(i, (kvl, kva)[i].at[d, tp], d, near[3]).wait_send()
            relay.wait_send()
    for g in range(GROUPS):
        first = 1 if g == 0 else 0
        part = obuf.at[g, pl.ds(first, PEERS - first)]
        remote(part, part, dsend.at[g], drecv.at[g], sp, other).wait_send()
        part = ybuf.at[g, tp, pl.ds(first, PEERS - first)]
        remote(part, part, bsend.at[g], brecv.at[g], sp, other).wait_send()
        remote(xbuf.at[g, tp], xbuf.at[g, tp], fsend.at[g], frecv.at[g], sp, other).wait_send()
        swap_of(g).wait_send()


def in_vmem():
    return pl.BlockSpec(memory_space=pltpu.VMEM)


def in_hbm():
    return pl.BlockSpec(memory_space=pltpu.HBM)


DMA = pltpu.SemaphoreType.DMA


def layer(*operands):
    return pl.pallas_call(
        layer_kernel,
        out_shape=jax.ShapeDtypeStruct((ROWS, D), BF16),
        in_specs=[in_hbm()] * 17,
        out_specs=in_vmem(),
        scratch_shapes=[
            pltpu.VMEM((TOK, RANK), BF16),
            pltpu.VMEM((DR, TOK), BF16),
            pltpu.VMEM((1, TOK), jnp.int32),
            pltpu.VMEM((1, 128), F32),
            pltpu.VMEM((1, D), F32),
            pltpu.VMEM((TOPK, ROWS), jnp.int32),
            pltpu.VMEM((TOPK, ROWS), F32),
            pltpu.VMEM((1, D), F32),
            pltpu.VMEM((TOK, LOCAL_HEADS * DK), BF16),
            pltpu.VMEM((TOK, LOCAL_HEADS * DR), BF16),
            pltpu.VMEM((ROWS, D), BF16),
            pltpu.VMEM((TOK, 128), BF16),
            pltpu.VMEM((TOK, LOCAL_HEADS * 128), BF16),
            pltpu.VMEM((REACH, 2, ROWS, RANK), BF16),
            pltpu.VMEM((REACH, 2, ROWS, 128), BF16),
            pltpu.VMEM((RANK, LOCAL_HEADS * DK), BF16),
            pltpu.VMEM((RANK, LOCAL_HEADS * DV), BF16),
            pltpu.VMEM((2, LOCAL_HEADS * DV, D), BF16),
            pltpu.VMEM((LOCAL_HEADS, TOK, 128), F32),
            pltpu.VMEM((LOCAL_HEADS, TOK, (REACH + 1) * TOK), F32),
            pltpu.VMEM(((REACH + 1) * TOK, LOCAL_HEADS * DV), BF16),
            pltpu.VMEM((TOK, LOCAL_HEADS * DV), BF16),
            pltpu.VMEM((ROWS, LOCAL_HEADS * DV), BF16),
            pltpu.VMEM((ROWS, D), BF16),
            pltpu.VMEM((D, FFH), BF16),
            pltpu.VMEM((D, FFH), BF16),
            pltpu.VMEM((FFH, D), BF16),
            pltpu.VMEM((GROUPS, PEERS, CAP, D), BF16),
            pltpu.VMEM((GROUPS, 2, PEERS, CAP, D), BF16),
            pltpu.VMEM((TOK, D), BF16),
            pltpu.VMEM((TOK, FFH), BF16),
            pltpu.VMEM((GROUPS, 2, PEERS, CAP, D), BF16),
            pltpu.VMEM((GROUPS, PEERS, CAP, D), BF16),
            pltpu.VMEM((GROUPS, PEERS, CAP, D), BF16),
            DMA((8,)),
            DMA((9,)),
        ]
        + [DMA((2, REACH))] * 4
        + [DMA((4,)), pltpu.SemaphoreType.REGULAR((2,))]
        + [DMA((GROUPS,))] * 8,
        compiler_params=pltpu.CompilerParams(
            collective_id=0, has_side_effects=True, vmem_limit_bytes=VMEM_LIMIT
        ),
    )(*operands)


def per_device(
    latent,
    rotary_key,
    doc_ids,
    queries_content,
    queries_rotary,
    w_key_up,
    w_value_up,
    w_out,
    residual,
    norm_gain,
    routes,
    route_weights,
    w_gate,
    w_up,
    w_down,
    out_gain,
):
    frequency = jnp.asarray(np.tile(ROPE_THETA ** (-2.0 * np.arange(DR // 2) / DR), 4), F32)
    mixed = layer(
        latent,
        rotary_key.T,
        doc_ids.reshape(1, TOK),
        frequency.reshape(1, 128),
        norm_gain.reshape(1, D),
        routes.T,
        route_weights.T,
        out_gain.reshape(1, D),
        queries_content,
        queries_rotary,
        residual,
        w_key_up,
        w_value_up,
        w_out,
        w_gate,
        w_up,
        w_down,
    )
    return mixed


def solution(mesh):
    return jax.shard_map(
        per_device,
        mesh=mesh,
        in_specs=(
            P("sp", None),
            P("sp", None),
            P("sp"),
            P("sp", "tp"),
            P("sp", "tp"),
            P(),
            P(),
            P("tp", None),
            P(("sp", "tp"), None),
            P(),
            P(("sp", "tp"), None),
            P(("sp", "tp"), None),
            P("sp", None, "tp"),
            P("sp", None, "tp"),
            P("sp", "tp", None),
            P(),
        ),
        out_specs=P(("sp", "tp"), None),
        check_vma=False,
    )
```
